128 devices in a mesh: sp: 32 (over z, y, core), tp: 4 (over x).
Axes of the slice: x: 4, y: 4, z: 4, core: 2. Of those that a mesh axis runs over, the one named last changes fastest.
Arguments:
- tokens: bfloat16 [16384, 2048], P('sp'), may hold values from -6 to 6
- input_norm_gain: bfloat16 [2048], replicated, may hold values from 0.099609375 to 1.8984375
- gate_matrix: bfloat16 [2048, 1024], P('sp', 'tp'), may hold values from -0.125 to 0.125
- input_matrix: bfloat16 [2048, 1024], P('sp', 'tp'), may hold values from -0.125 to 0.125
- write_matrix: bfloat16 [2048, 512], P('sp', 'tp'), may hold values from -0.125 to 0.125
- read_matrix: bfloat16 [2048, 512], P('sp', 'tp'), may hold values from -0.125 to 0.125
- step_matrix: bfloat16 [2048, 16], P('sp'), may hold values from -0.125 to 0.125
- pooling_input_matrix: bfloat16 [2048, 1024], P('sp', 'tp'), may hold values from -0.125 to 0.125
- input_conv_taps: bfloat16 [3, 1024], P(None, 'tp'), may hold values from -3.5 to 3.5
- write_conv_taps: bfloat16 [3, 512], P(None, 'tp'), may hold values from -3.5 to 3.5
- read_conv_taps: bfloat16 [3, 512], P(None, 'tp'), may hold values from -3.5 to 3.5
- head_step_base: float32 [16], P('tp'), may hold values from 0 to 1, as said below
- position_step_factor: float32 [16384], P('sp'), may hold values from 0 to 3, as said below
- position_log_decay: float32 [16384, 16], P('sp', 'tp'), may hold values from -2 to 0, as said below
- gated_norm_gain: bfloat16 [1024], P('tp'), may hold values from 0.099609375 to 1.8984375
- group_linear_maps: bfloat16 [4, 256, 256], P('tp'), may hold values from -0.375 to 0.375
- pooling_channel_scale: bfloat16 [1024], P('tp'), may hold values from 0.099609375 to 1.8984375
- state_output_matrix: bfloat16 [1024, 2048], P('tp', 'sp'), may hold values from -0.125 to 0.125
- pooling_output_matrix: bfloat16 [1024, 2048], P('tp', 'sp'), may hold values from -0.125 to 0.125
Outputs:
- mixed: bfloat16 [16384, 2048], P(('sp', 'tp'))
The draws below stay inside these ranges and needn't reach their ends.
Inputs may be any that keep to these rules, and one draw needn't show every extreme that they name: `head_step_base`: positive. `position_step_factor`: positive. `position_log_decay`: never positive.
All inputs are finite; a program needn't handle non-finite values.
Results may differ from the reference program's by a relative error of at most 0.012.
Values may be sent and summed in bfloat16 or wider, within the bound.
No kernel may reach another device: no remote copies, remote signals or barrier semaphores. Data moves between devices by JAX's collectives and lax.ppermute only.
A program may use at most 64 MiB of HBM per device.

```python
import jax
import jax.numpy as jnp
from jax import lax

D = 2048
SSD_INNER = 1024
HEAD_DIM = 64
GROUPS = 4
STATE = 128
POOL_WIDTH = 1024
POOL_GROUPS = 4
BLOCK = 128
TOK_DEV = 512
SSM_STREAMS = 16
PG = 256
TOKEN_TOTAL = 16384


def draw_tokens(key, part):
    key_noise, key_direction = jax.random.split(key, 2)
    segment = TOK_DEV // 2
    directions = jax.random.normal(key_direction, (TOKEN_TOTAL // segment, D), jnp.float32)
    noise = jax.random.normal(key_noise, (TOKEN_TOTAL, D), jnp.float32)
    offsets = directions
    return jnp.clip(noise + jnp.repeat(offsets, segment, axis=0), -6.0, 6.0).astype(jnp.bfloat16)


def draw_head_step_base(key, part):
    key_slow, key_fast, key_pick = jax.random.split(key, 3)
    slow_rates = jnp.exp(jax.random.uniform(key_slow, (SSM_STREAMS,), jnp.float32, jnp.log(0.1 / TOKEN_TOTAL), jnp.log(1.0 / TOKEN_TOTAL)))
    fast_rates = jnp.exp(jax.random.uniform(key_fast, (SSM_STREAMS,), jnp.float32, jnp.log(0.015), jnp.log(0.04)))
    ranking = jax.random.permutation(key_pick, SSM_STREAMS)
    chosen = ranking < SSM_STREAMS // 2
    return jnp.where(chosen, fast_rates, slow_rates)


def draw_position_step_factor(key, part):
    segment = TOK_DEV // 2
    factors = jnp.exp(jax.random.uniform(key, (TOKEN_TOTAL // segment,), jnp.float32, -0.7, 0.7))
    return jnp.repeat(factors, segment)


def draw_position_log_decay(key, part):
    key_spot, key_depth = jax.random.split(key, 2)
    site_offsets = jax.random.randint(key_spot, (4, SSM_STREAMS), 0, TOKEN_TOTAL)
    stack_levels = jax.random.uniform(key_depth, (4, SSM_STREAMS), jnp.float32, -0.5, -0.22)
    location_indices = jnp.arange(TOKEN_TOTAL)[:, None]
    fading_spans = jnp.zeros((TOKEN_TOTAL, SSM_STREAMS), jnp.float32)
    for entry_number in range(4):
        fading_spans = fading_spans + jnp.where(location_indices == site_offsets[entry_number][None, :], stack_levels[entry_number][None, :], 0.0)
    return fading_spans


def levels(stream_key, shape, cuts, least, top_value):
    def one(axis_at, parts):
        draws = jax.random.uniform(jax.random.fold_in(jax.random.fold_in(stream_key, 6), axis_at), (parts,), jnp.float32, least / len(cuts), top_value / len(cuts))
        return jnp.repeat(jnp.exp(draws), shape[axis_at] // parts).reshape((-1,) + (1,) * (len(shape) - axis_at - 1))

    loudness = one(*cuts[0])
    for cut in cuts[1:]:
        loudness = loudness * one(*cut)
    return loudness


def scatter_about(key, dims, deviation, bound, cuts=(), kind=jnp.bfloat16):
    factor_of = levels(key, dims, cuts, -0.22, 0.18) if cuts else 1.0
    result = jax.random.normal(key, dims, jnp.float32) * deviation * factor_of
    return jnp.minimum(jnp.maximum(result, -bound), bound).astype(kind)


def setup_inputs(seed: int = 0) -> dict:
    seeds = jax.random.split(jax.random.key(seed), 20)
    return {
        "tokens": draw_tokens(jax.random.fold_in(seeds[19], 71), 0),
        "input_norm_gain": jnp.clip(1.0 + 0.18 * jax.random.normal(seeds[1], (D,), jnp.float32), 0.099609375, 1.8984375).astype(jnp.bfloat16),
        "gate_matrix": scatter_about(seeds[2], (D, SSD_INNER), D ** -0.5, 0.125, ((0, 32), (1, 4))),
        "input_matrix": scatter_about(seeds[3], (D, SSD_INNER), D ** -0.5, 0.125, ((0, 32), (1, 4))),
        "write_matrix": scatter_about(seeds[4], (D, GROUPS * STATE), D ** -0.5, 0.125, ((0, 32), (1, 4))),
        "read_matrix": scatter_about(seeds[5], (D, GROUPS * STATE), D ** -0.5, 0.125, ((0, 32), (1, 4))),
        "step_matrix": scatter_about(seeds[6], (D, SSM_STREAMS), D ** -0.5, 0.125, ((0, 32),)),
        "pooling_input_matrix": scatter_about(seeds[7], (D, POOL_WIDTH), D ** -0.5, 0.125, ((0, 32), (1, 4))),
        "input_conv_taps": scatter_about(seeds[8], (3, SSD_INNER), 3 ** -0.5, 3.5, ((1, 4),)),
        "write_conv_taps": scatter_about(seeds[9], (3, GROUPS * STATE), 3 ** -0.5, 3.5, ((1, 4),)),
        "read_conv_taps": scatter_about(seeds[10], (3, GROUPS * STATE), 3 ** -0.5, 3.5, ((1, 4),)),
        "head_step_base": draw_head_step_base(jax.random.fold_in(seeds[19], 71), 0),
        "position_step_factor": draw_position_step_factor(jax.random.fold_in(seeds[19], 71), 0),
        "position_log_decay": draw_position_log_decay(jax.random.fold_in(seeds[19], 71), 0),
        "gated_norm_gain": jnp.clip(1.0 + 0.18 * jax.random.normal(seeds[14], (SSD_INNER,), jnp.float32), 0.099609375, 1.8984375).astype(jnp.bfloat16),
        "group_linear_maps": scatter_about(seeds[15], (POOL_GROUPS, PG, PG), PG ** -0.5, 0.375, ((0, 4),)),
        "pooling_channel_scale": jnp.clip(1.0 + 0.18 * jax.random.normal(seeds[16], (POOL_WIDTH,), jnp.float32), 0.099609375, 1.8984375).astype(jnp.bfloat16),
        "state_output_matrix": scatter_about(seeds[17], (SSD_INNER, D), (SSD_INNER + POOL_WIDTH) ** -0.5, 0.125, ((0, 4), (1, 32))),
        "pooling_output_matrix": scatter_about(seeds[18], (POOL_WIDTH, D), (SSD_INNER + POOL_WIDTH) ** -0.5, 0.125, ((0, 4), (1, 32))),
    }


EPSILON = 1e-06
HIGHEST_PRECISION = lax.Precision.HIGHEST

def block_sweep(readers, writers, values, decay_logarithm):
    length = values.shape[0]
    blocks = length // BLOCK
    lower_mask = jnp.tril(jnp.ones((BLOCK, BLOCK), dtype=bool))[:, :, None, None]

    def as_blocks(array):
        return array.reshape((blocks, BLOCK) + array.shape[1:])

    def one_block(carry_state, inputs):
        read_block, write_block, value_block, decay_block = inputs
        running = jnp.cumsum(decay_block, axis=0)
        scores = jnp.einsum('ign,jgn->ijg', read_block, write_block, precision=HIGHEST_PRECISION)
        spread = jnp.where(lower_mask, running[:, None] - running[None, :], -jnp.inf)
        weights = scores[..., None] * jnp.exp(spread)
        within = jnp.einsum('ijgr,jgrp->igrp', weights, value_block, precision=HIGHEST_PRECISION)
        carried = jnp.einsum('ign,grnp->igrp', read_block, carry_state, precision=HIGHEST_PRECISION)
        carried = carried * jnp.exp(running)[..., None]
        block_total = running[-1]
        fading = jnp.exp(block_total[None] - running)
        inflow = jnp.einsum('jgn,jgrp->grnp', write_block, value_block * fading[..., None], precision=HIGHEST_PRECISION)
        return (carry_state * jnp.exp(block_total)[..., None, None] + inflow, within + carried)
    initial = jnp.zeros((values.shape[1], values.shape[2], writers.shape[2], values.shape[3]), jnp.float32)
    last_state, outputs = lax.scan(one_block, initial, (as_blocks(readers), as_blocks(writers), as_blocks(values), as_blocks(decay_logarithm)))
    return (outputs.reshape(values.shape), last_state)

def centred_conv(signal, taps):
    length = signal.shape[0]
    padded = jnp.pad(signal, ((1, 1), (0, 0)))
    return padded[0:length] * taps[0] + padded[1:length + 1] * taps[1] + padded[2:length + 2] * taps[2]

def reference(tokens, input_norm_gain, gate_matrix, input_matrix, write_matrix, read_matrix, step_matrix, pooling_input_matrix, input_conv_taps, write_conv_taps, read_conv_taps, head_step_base, position_step_factor, position_log_decay, gated_norm_gain, group_linear_maps, pooling_channel_scale, state_output_matrix, pooling_output_matrix):
    f32 = jnp.float32
    bf16 = jnp.bfloat16
    wide = tokens.astype(f32)
    normed = (wide * lax.rsqrt(lax.optimization_barrier(jnp.mean(wide * wide, axis=1, keepdims=True)) + EPSILON) * input_norm_gain.astype(f32)).astype(bf16)

    def project(weight):
        return jnp.dot(normed, weight, preferred_element_type=f32)
    gate_pre = project(gate_matrix).astype(bf16)
    input_pre = project(input_matrix).astype(bf16)
    write_pre = project(write_matrix).astype(bf16)
    read_pre = project(read_matrix).astype(bf16)
    pool_in = project(pooling_input_matrix).astype(bf16)
    step_raw = project(step_matrix)
    inputs = jax.nn.silu(centred_conv(input_pre.astype(f32), input_conv_taps.astype(f32))).astype(bf16)
    writers = jax.nn.silu(centred_conv(write_pre.astype(f32), write_conv_taps.astype(f32))).astype(bf16)
    readers = jax.nn.silu(centred_conv(read_pre.astype(f32), read_conv_taps.astype(f32))).astype(bf16)
    step_size = head_step_base[None, :] * jax.nn.softplus(step_raw) * position_step_factor[:, None]
    decay_logarithm = position_log_decay - step_size
    repeat_count = SSM_STREAMS // GROUPS
    values = (inputs.astype(f32).reshape(TOKEN_TOTAL, SSM_STREAMS, HEAD_DIM) * step_size[..., None]).reshape(TOKEN_TOTAL, GROUPS, repeat_count, HEAD_DIM)
    grouped_decay = decay_logarithm.reshape(TOKEN_TOTAL, GROUPS, repeat_count)
    readers_f = readers.astype(f32).reshape(TOKEN_TOTAL, GROUPS, STATE)
    writers_f = writers.astype(f32).reshape(TOKEN_TOTAL, GROUPS, STATE)
    ahead, unused_a = block_sweep(readers_f, writers_f, values, grouped_decay)
    behind, unused_b = block_sweep(jnp.flip(readers_f, 0), jnp.flip(writers_f, 0), jnp.flip(values, 0), jnp.flip(grouped_decay, 0))
    scanned = (ahead + jnp.flip(behind, 0)).reshape(TOKEN_TOTAL, SSD_INNER)
    gated = scanned * jax.nn.silu(gate_pre.astype(f32))
    state_mixed = (gated * lax.rsqrt(lax.optimization_barrier(jnp.mean(gated * gated, axis=1, keepdims=True)) + EPSILON) * gated_norm_gain.astype(f32)).astype(bf16)
    width_group = POOL_WIDTH // POOL_GROUPS
    reach = 2 ** (POOL_GROUPS - 1)
    grouped_in = pool_in.astype(f32).reshape(TOKEN_TOTAL, POOL_GROUPS, width_group)
    extended = jnp.pad(grouped_in, ((reach, reach), (0, 0), (0, 0)))
    halves = 2 ** jnp.arange(POOL_GROUPS)
    window_sum = jnp.zeros_like(grouped_in)
    for offset in range(-reach, reach):
        taken = ((offset >= -halves) & (offset < halves)).astype(f32)
        window_sum = window_sum + extended[reach + offset:reach + offset + TOKEN_TOTAL] * taken[None, :, None]
    positions = jnp.arange(TOKEN_TOTAL)[:, None]
    counts = (jnp.minimum(positions + halves[None, :], TOKEN_TOTAL) - jnp.maximum(positions - halves[None, :], 0)).astype(f32)
    pooled = (window_sum / counts[..., None] - grouped_in).astype(bf16)
    mapped = jnp.einsum('tgc,gcd->tgd', pooled.astype(f32), group_linear_maps.astype(f32))
    pool_mixed = (mapped.reshape(TOKEN_TOTAL, POOL_WIDTH) * pooling_channel_scale.astype(f32)).astype(bf16)
    summed = jnp.dot(state_mixed, state_output_matrix, preferred_element_type=f32) + jnp.dot(pool_mixed, pooling_output_matrix, preferred_element_type=f32)
    return summed.astype(bf16)
```

```python
import functools

import jax
import jax.numpy as jnp
from jax import lax
from jax.experimental import pallas as pl
from jax.experimental.pallas import tpu as pltpu
from jax.sharding import Mesh, PartitionSpec as P

EPSILON = 1e-06
SSD_INNER = 1024
TOKEN_TOTAL = 16384
LOCAL = 512
CHUNK = 1024
HALO = 8
ROWS = CHUNK + 2 * HALO
BLOCK = 256
BLOCKS = CHUNK // BLOCK
LANES = 128
CHIPS = 16

f32 = jnp.float32
bf16 = jnp.bfloat16


VMEM = pl.BlockSpec(memory_space=pltpu.VMEM)
SMEM = pl.BlockSpec(memory_space=pltpu.SMEM)


def call(kernel, outs, args, name, smem=0):
    return pl.pallas_call(
        kernel,
        out_shape=[jax.ShapeDtypeStruct(s, d) for s, d in outs],
        in_specs=[SMEM] * smem + [VMEM] * (len(args) - smem),
        out_specs=[VMEM] * len(outs),
        name=name,
        compiler_params=pltpu.CompilerParams(vmem_limit_bytes=56 * 1024 * 1024),
    )(*args)


def dot(a, b):
    return lax.dot_general(a, b, (((1,), (0,)), ((), ())), preferred_element_type=f32)


def dot_nt(a, b):
    return lax.dot_general(a, b, (((1,), (1,)), ((), ())), preferred_element_type=f32)


def dot_tn(a, b):
    return lax.dot_general(a, b, (((0,), (0,)), ((), ())), preferred_element_type=f32)


def pieces(value):
    high = value.astype(bf16)
    rest = value - high.astype(f32)
    mid = rest.astype(bf16)
    low = (rest - mid.astype(f32)).astype(bf16)
    return high, mid, low


def silu(value):
    return value / (1.0 + jnp.exp(-value))


def first_kernel(normed, recv, taps, base, acted, raw, pre):
    weight = jnp.concatenate(
        [recv[:, 0:64, :].reshape(2048, LANES), recv[:, 64:128, :].reshape(2048, LANES)], axis=1
    )
    for at, size in ((0, 264), (264, 256), (520, 256), (776, 264)):
        got = dot(normed[at : at + size, :], weight)
        pre[at : at + size, :] = got.astype(bf16).astype(f32)
    steps = recv[:, 128:136, :].astype(f32).reshape(16, 2, 8, LANES)
    steps = (steps[:, 0] + steps[:, 1]).astype(bf16)
    rows = jnp.concatenate([steps[k] for k in range(16)], axis=1)
    first = jnp.broadcast_to(rows[0:1], (64, 2048))
    second = jnp.broadcast_to(rows[1:2], (64, 2048))
    spread = jnp.concatenate([first, second], axis=0)
    for at in range(0, CHUNK, BLOCK):
        raw[at : at + BLOCK, :] = dot_nt(normed[HALO + at : HALO + at + BLOCK, :], spread)
        out = (
            pre[HALO - 1 + at : HALO - 1 + at + BLOCK, :] * taps[0:1, :]
            + pre[HALO + at : HALO + at + BLOCK, :] * taps[1:2, :]
            + pre[HALO + 1 + at : HALO + 1 + at + BLOCK, :] * taps[2:3, :]
        )
        acted[at : at + BLOCK, :] = silu(out).astype(bf16)


def decay_kernel(inputs, raw, position, base, values, scaled, running, entry, totals):
    lane = lax.broadcasted_iota(jnp.int32, (BLOCK, LANES), 1)
    rows = lax.broadcasted_iota(jnp.int32, (BLOCK, BLOCK), 0)
    cols = lax.broadcasted_iota(jnp.int32, (BLOCK, BLOCK), 1)
    lower = jnp.where(cols <= rows, 1.0, 0.0).astype(bf16)
    sums = []
    for at in range(0, CHUNK, BLOCK):
        here = pl.ds(at, BLOCK)
        r = raw[here, :]
        soft = jnp.maximum(r, 0.0) + jnp.log1p(jnp.exp(-jnp.abs(r)))
        step = base[0:1, :] * soft * position[here, 2:3]
        fall = jnp.where(lane < 64, position[here, 0:1], position[here, 1:2]) - step
        total = sum(dot(lower, piece) for piece in pieces(fall))
        start = total - fall
        end = total[BLOCK - 1 : BLOCK, :]
        value = inputs[here, :].astype(f32) * step
        values[here, :] = value.astype(bf16)
        scaled[here, 0:LANES] = (value * jnp.exp(end - total)).astype(bf16)
        scaled[here, LANES:] = (value * jnp.exp(start)).astype(bf16)
        running[here, :] = total
        entry[here, :] = start
        sums.append(end)
    totals[...] = jnp.concatenate(sums + [jnp.zeros((8 - BLOCKS, LANES), f32)], axis=0)


def state_kernel(me, writers, scaled, totals, slots, ahead, behind):
    parts = []
    for b in range(BLOCKS):
        here = pl.ds(b * BLOCK, BLOCK)
        parts.append(dot_tn(writers[here, :], scaled[here, :]))
    state = jnp.zeros((LANES, LANES), f32)
    for b in range(BLOCKS):
        ahead[b] = state
        state = state * jnp.exp(totals[b : b + 1, :]) + parts[b][:, :LANES]
    back = jnp.zeros((LANES, LANES), f32)
    for b in reversed(range(BLOCKS)):
        behind[b] = back
        back = back * jnp.exp(totals[b : b + 1, :]) + parts[b][:, LANES:]
    total = totals[0:1, :]
    for b in range(1, BLOCKS):
        total = total + totals[b : b + 1, :]
    row = lax.broadcasted_iota(jnp.int32, (8, LANES), 0)
    high, mid, low = (p.astype(f32) for p in pieces(total))
    tail = jnp.where(row == 0, high, jnp.where(row == 1, mid, jnp.where(row == 2, low, 0.0)))
    tail = tail.astype(bf16)
    state = state.astype(bf16)
    back = back.astype(bf16)
    for j in range(CHIPS):
        slots[j, 0:LANES, :] = jnp.where(j > me[0], state, back)
        slots[j, LANES : LANES + 8, :] = tail


def local_kernel(readers, writers, values, running, entry, out):
    rows = lax.broadcasted_iota(jnp.int32, (BLOCK, BLOCK), 0)
    cols = lax.broadcasted_iota(jnp.int32, (BLOCK, BLOCK), 1)
    lane = lax.broadcasted_iota(jnp.int32, (BLOCK, LANES), 1)
    for b in range(BLOCKS):
        here = pl.ds(b * BLOCK, BLOCK)
        scores = dot_nt(readers[here, :], writers[here, :])
        total = running[here, :]
        start = entry[here, :]
        total_t = total.T
        start_t = start.T
        result = jnp.zeros((BLOCK, LANES), f32)
        for h in range(2):
            at = h * 64
            gap = jnp.where(
                cols < rows,
                total[:, at : at + 1] - total_t[at : at + 1, :],
                start_t[at : at + 1, :] - start[:, at : at + 1],
            )
            weight = jnp.exp(jnp.minimum(gap, 0.0))
            weight = jnp.where(cols == rows, 2.0, weight)
            own = jnp.where((lane < 64) == (h == 0), values[here, :], jnp.zeros((), bf16))
            result = result + dot((scores * weight).astype(bf16), own)
        out[here, :] = result


def second_kernel(group, place, normed, recv, gate, pooled, pre):
    weight = jnp.concatenate(
        [recv[:, 0:64, :].reshape(2048, LANES), recv[:, 64:128, :].reshape(2048, LANES)], axis=1
    )
    for at, size in ((0, 264), (264, 256), (520, 256), (776, 264)):
        pre[at : at + size, :] = dot(normed[at : at + size, :], weight)
    g = group[0]
    half = jnp.where(g == 0, 1, jnp.where(g == 1, 2, jnp.where(g == 2, 4, 8)))
    for at in range(0, CHUNK, BLOCK):
        here = pl.ds(at, BLOCK)
        gate[here, :] = silu(pre[HALO + at : HALO + at + BLOCK, 0:LANES].astype(bf16).astype(f32))

        def taken(offset):
            return pre[HALO + at + offset : HALO + at + offset + BLOCK, LANES:]

        own = taken(0)
        two = taken(-1) + own
        four = two + taken(-2) + taken(1)
        eight = four + taken(-4) + taken(-3) + taken(2) + taken(3)
        wide = eight
        for offset in (-8, -7, -6, -5, 4, 5, 6, 7):
            wide = wide + taken(offset)
        window = jnp.where(g == 0, two, jnp.where(g == 1, four, jnp.where(g == 2, eight, wide)))
        token = place[0] * CHUNK + at + lax.broadcasted_iota(jnp.int32, (BLOCK, LANES), 0)
        count = jnp.minimum(token + half, TOKEN_TOTAL) - jnp.maximum(token - half, 0)
        pooled[here, :] = (window / count.astype(f32) - own).astype(bf16)


def enter_kernel(me, recv, readers, local, gate, running, entry, totals, ahead, behind, pooled, out):
    decays = []
    for j in range(CHIPS):
        decays.append(jnp.sum(recv[j, LANES : LANES + 8, :].astype(f32), axis=0, keepdims=True))
    entering = jnp.zeros((LANES, LANES), f32)
    for j in range(CHIPS):
        used = jnp.where(j < me[0], 1.0, 0.0)
        entering = entering * jnp.exp(decays[j] * used) + recv[j, 0:LANES, :].astype(f32) * used
    leaving = jnp.zeros((LANES, LANES), f32)
    for j in reversed(range(CHIPS)):
        used = jnp.where(j > me[0], 1.0, 0.0)
        leaving = leaving * jnp.exp(decays[j] * used) + recv[j, 0:LANES, :].astype(f32) * used
    before = [jnp.zeros((1, LANES), f32)]
    for b in range(BLOCKS):
        before.append(before[-1] + totals[b : b + 1, :])
    for b in range(BLOCKS):
        here = pl.ds(b * BLOCK, BLOCK)
        left = (ahead[b] + entering * jnp.exp(before[b])).astype(bf16)
        right = (behind[b] + leaving * jnp.exp(before[BLOCKS] - before[b + 1])).astype(bf16)
        both = dot(readers[here, :], jnp.concatenate([left, right], axis=1))
        scanned = (
            local[here, :]
            + both[:, :LANES] * jnp.exp(running[here, :])
            + both[:, LANES:] * jnp.exp(totals[b : b + 1, :] - entry[here, :])
        )
        gated = (scanned * gate[here, :]).astype(bf16)
        for k in range(BLOCK // LANES):
            slot = b * (BLOCK // LANES) + k
            out[slot, 0:LANES, :] = gated[k * LANES : (k + 1) * LANES, :]
            out[slot, LANES:, :] = pooled[slot * LANES : (slot + 1) * LANES, :]


def last_kernel(recv, weight, out):
    gated = [recv[j, 0:LANES, :] for j in range(8)]
    pooled = [recv[j, LANES:, :] for j in range(8)]
    squares = sum(
        jnp.sum(g.astype(f32) * g.astype(f32), axis=1, keepdims=True) for g in gated
    )
    factor = lax.rsqrt(squares / SSD_INNER + EPSILON)
    state = 0.0
    pool = 0.0
    for x in range(4):
        state = state + dot_nt(
            jnp.concatenate([gated[x], gated[4 + x]], axis=1), weight[x, :, 0:256]
        )
        pool = pool + dot_nt(
            jnp.concatenate([pooled[x], pooled[4 + x]], axis=1), weight[x, :, 256:512]
        )
    out[...] = (state * factor + pool).astype(bf16)


def shards(
    tokens,
    input_norm_gain,
    gate_matrix,
    input_matrix,
    write_matrix,
    read_matrix,
    step_matrix,
    pooling_input_matrix,
    input_conv_taps,
    write_conv_taps,
    read_conv_taps,
    head_step_base,
    position_step_factor,
    position_log_decay,
    gated_norm_gain,
    group_linear_maps,
    pooling_channel_scale,
    state_output_matrix,
    pooling_output_matrix,
):
    core = lax.axis_index("c")
    group = lax.axis_index("x")
    chip = lax.axis_index(("z", "y"))
    swap = [(0, 1), (1, 0)]

    def halves(array):
        return jnp.stack([array[..., :LANES], array[..., LANES:]])

    scaled_state = (state_output_matrix.astype(f32) * gated_norm_gain.astype(f32)[:, None]).astype(
        bf16
    )
    columns = jnp.concatenate([scaled_state, pooling_output_matrix], axis=0).T
    out_weight = lax.all_gather(columns, ("x", "z", "y", "c"), axis=0, tiled=True)
    out_weight = out_weight.reshape(4, 2048, 512)

    own_steps = lax.dynamic_slice_in_dim(step_matrix, group * 4, 4, 1).T.reshape(2, 2, 64)
    none = jnp.zeros_like(own_steps)
    own_steps = jnp.concatenate(
        [jnp.where(core == 0, own_steps, none), jnp.where(core == 0, none, own_steps)], axis=2
    )
    own_steps = jnp.pad(own_steps, ((0, 0), (0, 6), (0, 0)))
    part_a = jnp.concatenate(
        [halves(input_matrix), jnp.stack([write_matrix, read_matrix]), own_steps], axis=1
    )
    folded = (
        jnp.dot(pooling_input_matrix, group_linear_maps[0], preferred_element_type=f32)
        * pooling_channel_scale.astype(f32)[None, :]
    ).astype(bf16)
    part_b = jnp.concatenate([halves(gate_matrix), halves(folded)], axis=1)

    def exchanged(part):
        rows = part.shape[1]
        whole = jnp.broadcast_to(part[None], (CHIPS, 2, rows, LANES)).reshape(32, rows, LANES)
        return lax.all_to_all(whole, ("z", "y", "c"), 0, 0, tiled=True)

    recv_a = exchanged(part_a)
    part_b, recv_a = lax.optimization_barrier((part_b, recv_a))
    recv_b = exchanged(part_b)

    other = lax.ppermute(tokens, "c", swap)
    both = jnp.concatenate(
        [jnp.where(core == 0, tokens, other), jnp.where(core == 0, other, tokens)], axis=0
    )
    up = [(i, i + 1) for i in range(CHIPS - 1)]
    down = [(i + 1, i) for i in range(CHIPS - 1)]
    before = lax.ppermute(both[CHUNK - HALO :], ("z", "y"), up)
    after = lax.ppermute(both[:HALO], ("z", "y"), down)
    wide = jnp.concatenate([before, both, after], axis=0).astype(f32)
    normed = (
        wide
        * lax.rsqrt(jnp.mean(wide * wide, axis=1, keepdims=True) + EPSILON)
        * input_norm_gain.astype(f32)
    ).astype(bf16)

    places = jnp.concatenate(
        [position_log_decay.T, position_step_factor[None], jnp.zeros((3, LOCAL), f32)], axis=0
    )
    other_places = lax.ppermute(places, "c", swap)
    places = jnp.concatenate(
        [
            jnp.where(core == 0, places, other_places),
            jnp.where(core == 0, other_places, places),
        ],
        axis=1,
    )
    position = jnp.concatenate(
        [lax.dynamic_slice_in_dim(places, core * 2, 2, 0), places[4:5]], axis=0
    ).T
    base = jnp.repeat(lax.dynamic_slice_in_dim(head_step_base, core * 2, 2, 0), 64)[None]
    taps_in = lax.dynamic_slice_in_dim(input_conv_taps, core * LANES, LANES, 1)
    taps_wr = jnp.where(core == 0, write_conv_taps, read_conv_taps)
    taps = jnp.concatenate([taps_in, taps_wr], axis=1).astype(f32)

    acted, raw = pl.pallas_call(
        lambda n, r, t, a, w, p: first_kernel(n, r, t, None, a, w, p),
        out_shape=[
            jax.ShapeDtypeStruct((CHUNK, 256), bf16),
            jax.ShapeDtypeStruct((CHUNK, LANES), f32),
        ],
        in_specs=[VMEM] * 3,
        out_specs=[VMEM] * 2,
        scratch_shapes=[pltpu.VMEM((ROWS, 256), f32)],
        name="first",
        compiler_params=pltpu.CompilerParams(vmem_limit_bytes=56 * 1024 * 1024),
    )(normed, recv_a, taps)
    mine = acted[:, LANES:]
    theirs = lax.ppermute(mine, "c", swap)
    values, scaled, running, entry, totals = call(
        decay_kernel,
        [
            ((CHUNK, LANES), bf16),
            ((CHUNK, 256), bf16),
            ((CHUNK, LANES), f32),
            ((CHUNK, LANES), f32),
            ((8, LANES), f32),
        ],
        (acted[:, :LANES], raw, position, base),
        "decay",
    )
    writers = jnp.where(core == 0, mine, theirs)
    readers = jnp.where(core == 0, theirs, mine)
    me = chip.astype(jnp.int32).reshape(1)
    slots, ahead, behind = call(
        state_kernel,
        [
            ((CHIPS, LANES + 8, LANES), bf16),
            ((BLOCKS, LANES, LANES), f32),
            ((BLOCKS, LANES, LANES), f32),
        ],
        (me, writers, scaled, totals),
        "states",
        smem=1,
    )
    slots, recv_b = lax.optimization_barrier((slots, recv_b))
    recv_state = lax.all_to_all(slots, ("z", "y"), 0, 0, tiled=True)
    (local,) = call(
        local_kernel,
        [((CHUNK, LANES), f32)],
        (readers, writers, values, running, entry),
        "local",
    )
    gate, pooled = pl.pallas_call(
        second_kernel,
        out_shape=[
            jax.ShapeDtypeStruct((CHUNK, LANES), f32),
            jax.ShapeDtypeStruct((CHUNK, LANES), bf16),
        ],
        in_specs=[SMEM] * 2 + [VMEM] * 2,
        out_specs=[VMEM] * 2,
        scratch_shapes=[pltpu.VMEM((ROWS, 256), f32)],
        name="second",
        compiler_params=pltpu.CompilerParams(vmem_limit_bytes=56 * 1024 * 1024),
    )(group.astype(jnp.int32).reshape(1), me, normed, recv_b)
    (sent,) = call(
        enter_kernel,
        [((8, 2 * LANES, LANES), bf16)],
        (me, recv_state, readers, local, gate, running, entry, totals, ahead, behind, pooled),
        "enter",
        smem=1,
    )
    recv = lax.all_to_all(sent, ("c", "x"), 0, 0, tiled=True)
    width = 512
    return pl.pallas_call(
        last_kernel,
        out_shape=jax.ShapeDtypeStruct((LANES, 2048), bf16),
        grid=(2048 // width,),
        in_specs=[
            pl.BlockSpec((8, 2 * LANES, LANES), lambda i: (0, 0, 0)),
            pl.BlockSpec((4, width, 512), lambda i: (0, i, 0)),
        ],
        out_specs=pl.BlockSpec((LANES, width), lambda i: (0, i)),
        name="last",
        compiler_params=pltpu.CompilerParams(vmem_limit_bytes=40 * 1024 * 1024),
    )(recv, out_weight)


def solution(mesh):
    split = Mesh(mesh.devices.reshape(4, 4, 2, 4), ("z", "y", "c", "x"))
    sp = ("z", "y", "c")
    placed = (
        P(sp, None),
        P(),
        P(sp, "x"),
        P(sp, "x"),
        P(sp, "x"),
        P(sp, "x"),
        P(sp, None),
        P(sp, "x"),
        P(None, "x"),
        P(None, "x"),
        P(None, "x"),
        P("x"),
        P(sp),
        P(sp, "x"),
        P("x"),
        P("x", None, None),
        P("x"),
        P("x", sp),
        P("x", sp),
    )
    return jax.shard_map(
        shards,
        mesh=split,
        in_specs=placed,
        out_specs=P(("z", "y", "c", "x"), None),
        check_vma=False,
    )
```

```python
import jax
import jax.numpy as jnp
from jax import lax
from jax.experimental import pallas as pl
from jax.experimental.pallas import tpu as pltpu
from jax.sharding import Mesh, PartitionSpec as P

EPSILON = 1e-06
SSD_INNER = 1024
TOKEN_TOTAL = 16384
LOCAL = 512
CHUNK = 1024
HALO = 8
ROWS = CHUNK + 2 * HALO
BLOCK = 256
BLOCKS = CHUNK // BLOCK
LANES = 128
CHIPS = 16
STEPS = 8

f32 = jnp.float32
bf16 = jnp.bfloat16


VMEM = pl.BlockSpec(memory_space=pltpu.VMEM)
SMEM = pl.BlockSpec(memory_space=pltpu.SMEM)


def call(kernel, outs, args, name, smem=1, scratch=(), near=(), far=(), far_outs=(), raw_in=()):
    n_in, n_out = len(args), len(outs)
    far, far_outs = tuple(far), tuple(far_outs)
    placed = []
    for i, a in enumerate(args):
        if i in near:
            a = pltpu.with_memory_space_constraint(a, pltpu.VMEM)
        elif i in far:
            a = pltpu.with_memory_space_constraint(a, pltpu.HBM)
        placed.append(a)
    hbm = pl.BlockSpec(memory_space=pltpu.HBM)

    def body(*refs):
        ins, rest = list(refs[:n_in]), refs[n_in:]
        results, rest = list(rest[:n_out]), rest[n_out:]
        own, rest = rest[: len(scratch)], rest[len(scratch) :]
        spaces, flags = rest[:-1], rest[-1]
        copies = []
        for k, i in enumerate(far):
            copies.append(pltpu.make_async_copy(ins[i], spaces[k], flags.at[k]))
            ins[i] = spaces[k]
        for c in copies:
            c.start()
        backs = []
        for k, i in enumerate(far_outs):
            space = spaces[len(far) + k]
            backs.append(pltpu.make_async_copy(space, results[i], flags.at[len(far) + k]))
            results[i] = space
        for c in copies:
            c.wait()
        kernel(*ins, *results, *own)
        for c in backs:
            c.start()
        for c in backs:
            c.wait()

    spaces = [pltpu.VMEM(args[i].shape, args[i].dtype) for i in far]
    spaces += [pltpu.VMEM(*outs[i]) for i in far_outs]
    return pl.pallas_call(
        body,
        out_shape=[
            pltpu.HBM(s, d) if i in far_outs else pltpu.VMEM(s, d)
            for i, (s, d) in enumerate(outs)
        ],
        in_specs=[
            SMEM if i < smem else hbm if i in far or i in raw_in else VMEM
            for i in range(n_in)
        ],
        out_specs=[hbm if i in far_outs else VMEM for i in range(n_out)],
        scratch_shapes=list(scratch)
        + spaces
        + [pltpu.SemaphoreType.DMA((max(1, len(far) + len(far_outs)),))],
        name=name,
        compiler_params=pltpu.CompilerParams(vmem_limit_bytes=24 * 1024 * 1024),
    )(*placed)


def dot(a, b):
    return lax.dot_general(a, b, (((1,), (0,)), ((), ())), preferred_element_type=f32)


def dot_nt(a, b):
    return lax.dot_general(a, b, (((1,), (1,)), ((), ())), preferred_element_type=f32)


def dot_tn(a, b):
    return lax.dot_general(a, b, (((0,), (0,)), ((), ())), preferred_element_type=f32)


def pieces(value):
    high = value.astype(bf16)
    rest = value - high.astype(f32)
    mid = rest.astype(bf16)
    low = (rest - mid.astype(f32)).astype(bf16)
    return high, mid, low


def silu(value):
    return value / (1.0 + jnp.exp(-value))


def prepare_kernel(
    place, inputs, write, read, gates, pools, maps, scale, steps, sent, turned
):
    core, group = place[0], place[1]
    turned[...] = steps[...].astype(f32)
    folded = (dot(pools[...], maps[0]) * scale[...].astype(f32)).astype(bf16)
    row = lax.broadcasted_iota(jnp.int32, (8, LANES), 0)
    lane = lax.broadcasted_iota(jnp.int32, (8, LANES), 1)
    for c in range(2):
        at = group * 4 + 2 * c
        here = slice(c * LANES, (c + 1) * LANES)
        pair = [jnp.concatenate([turned[pl.ds(at + h, 1), :]] * 2, axis=1) for h in range(2)]
        tail = jnp.where(row == 0, pair[0], jnp.where(row == 1, pair[1], 0.0))
        tail = jnp.where((lane < 64) == (core == 0), tail, 0.0).astype(bf16)
        for j in range(CHIPS):
            sent[2 * j + c, 0:64, :] = inputs[:, here]
            sent[2 * j + c, 64:128, :] = (write, read)[c][...]
            sent[2 * j + c, 128:192, :] = gates[:, here]
            sent[2 * j + c, 192:256, :] = folded[:, here]
            sent[2 * j + c, 256:264, :] = tail


def normal(rows, scale):
    wide = rows.astype(f32)
    mean = jnp.mean(wide * wide, axis=1, keepdims=True)
    return (wide * lax.rsqrt(mean + EPSILON) * scale).astype(bf16)


def norm_kernel(place, own, other, gain, out):
    core = place[0]
    scale = gain[...].astype(f32)

    def body(k, carry):
        for source, half in ((own, core), (other, 1 - core)):
            rows = normal(source[pl.ds(pl.multiple_of(k * 64, 64), 64), :], scale)
            here = pl.ds(pl.multiple_of(half * LOCAL + k * 64, 64), 64)
            out[here, :] = rows
        return carry

    lax.fori_loop(0, LOCAL // 64, body, 0)


def project(normed, edges, weight, pre, rounded, copies=()):
    def keep(value):
        return value.astype(bf16).astype(f32) if rounded else value

    for at in range(0, CHUNK, BLOCK):
        for c in copies[at // BLOCK : at // BLOCK + 1]:
            c.wait()
        pre[HALO + at : HALO + at + BLOCK, :] = keep(dot(normed[at : at + BLOCK, :], weight))
    edge = keep(dot(edges, weight))
    pre[0:HALO, :] = edge[0:HALO]
    pre[HALO + CHUNK :, :] = edge[HALO:]


def first_kernel(
    source, recv, taps, before, after, gain, inputs, mine, raw, again, later, edges, pre, normed, flags
):
    copies = [
        pltpu.make_async_copy(
            source.at[pl.ds(at, BLOCK), :], normed.at[pl.ds(at, BLOCK), :], flags.at[at // BLOCK]
        )
        for at in range(0, CHUNK, BLOCK)
    ]
    for c in copies:
        c.start()
    weight = jnp.concatenate(
        [recv[:, 0:64, :].reshape(2048, LANES), recv[:, 64:128, :].reshape(2048, LANES)], axis=1
    )
    rows = jnp.concatenate([before[...], after[...]], axis=0)
    edge = normal(rows, gain[...].astype(f32))
    edges[...] = edge
    project(normed, edge, weight, pre, True, copies)
    steps = recv[:, 256:264, :].astype(f32).reshape(16, 2, 8, LANES)
    steps = (steps[:, 0] + steps[:, 1]).astype(bf16)
    rows = jnp.concatenate([steps[k] for k in range(16)], axis=1)
    first = jnp.broadcast_to(rows[0:1], (64, 2048))
    second = jnp.broadcast_to(rows[1:2], (64, 2048))
    spread = jnp.concatenate([first, second], axis=0)
    for at in range(0, CHUNK, BLOCK):
        step = dot_nt(normed[at : at + BLOCK, :], spread)
        raw[at : at + BLOCK, :] = step
        later[at : at + BLOCK, :] = step
        out = (
            pre[HALO - 1 + at : HALO - 1 + at + BLOCK, :] * taps[0:1, :]
            + pre[HALO + at : HALO + at + BLOCK, :] * taps[1:2, :]
            + pre[HALO + 1 + at : HALO + 1 + at + BLOCK, :] * taps[2:3, :]
        )
        out = silu(out).astype(bf16)
        inputs[at : at + BLOCK, :] = out[:, :LANES]
        again[at : at + BLOCK, :] = out[:, :LANES]
        mine[at : at + BLOCK, :] = out[:, LANES:]


def decays(core, raw, own, other, base):
    lane = lax.broadcasted_iota(jnp.int32, (BLOCK, LANES), 1)
    rows = lax.broadcasted_iota(jnp.int32, (BLOCK, BLOCK), 0)
    cols = lax.broadcasted_iota(jnp.int32, (BLOCK, BLOCK), 1)
    lower = jnp.where(cols <= rows, 1.0, 0.0).astype(bf16)
    places = [jnp.where(core == 0, own[...], other[...]), jnp.where(core == 0, other[...], own[...])]
    places = [p.T for p in places]
    for at in range(0, CHUNK, BLOCK):
        position = places[at // LOCAL][at % LOCAL : at % LOCAL + BLOCK, :]
        falls = jnp.where(core == 0, position[:, 0:2], position[:, 2:4])
        r = raw[at : at + BLOCK, :]
        soft = jnp.maximum(r, 0.0) + jnp.log1p(jnp.exp(-jnp.abs(r)))
        step = base[0:1, :] * soft * position[:, 4:5]
        fall = jnp.where(lane < 64, falls[:, 0:1], falls[:, 1:2]) - step
        total = sum(dot(lower, piece) for piece in pieces(fall))
        yield step, total, total - fall


def decay_kernel(place, inputs, raw, own, other, base, scaled, totals):
    sums = []
    for b, (step, total, start) in enumerate(decays(place[0], raw, own, other, base)):
        here = pl.ds(b * BLOCK, BLOCK)
        end = total[BLOCK - 1 : BLOCK, :]
        value = inputs[here, :].astype(f32) * step
        scaled[here, 0:LANES] = (value * jnp.exp(end - total)).astype(bf16)
        scaled[here, LANES:] = (value * jnp.exp(start)).astype(bf16)
        sums.append(end)
    totals[...] = jnp.concatenate(sums + [jnp.zeros((8 - BLOCKS, LANES), f32)], axis=0)


def state_kernel(place, mine, theirs, scaled, totals, slots, ahead, behind):
    parts = []
    for b in range(BLOCKS):
        here = pl.ds(b * BLOCK, BLOCK)
        writers = jnp.where(place[0] == 0, mine[here, :], theirs[here, :])
        parts.append(dot_tn(writers, scaled[here, :]))
    state = jnp.zeros((LANES, LANES), f32)
    for b in range(BLOCKS):
        ahead[b] = state
        state = state * jnp.exp(totals[b : b + 1, :]) + parts[b][:, :LANES]
    back = jnp.zeros((LANES, LANES), f32)
    for b in reversed(range(BLOCKS)):
        behind[b] = back
        back = back * jnp.exp(totals[b : b + 1, :]) + parts[b][:, LANES:]
    total = totals[0:1, :]
    for b in range(1, BLOCKS):
        total = total + totals[b : b + 1, :]
    row = lax.broadcasted_iota(jnp.int32, (8, LANES), 0)
    high, mid, low = (p.astype(f32) for p in pieces(total))
    tail = jnp.where(row == 0, high, jnp.where(row == 1, mid, jnp.where(row == 2, low, 0.0)))
    tail = tail.astype(bf16)
    state = state.astype(bf16)
    back = back.astype(bf16)
    for j in range(CHIPS):
        slots[j, 0:LANES, :] = jnp.where(j > place[2], state, back)
        slots[j, LANES : LANES + 8, :] = tail


def middle_kernel(
    place,
    normed,
    edges,
    recv,
    mine,
    theirs,
    inputs,
    raw,
    own,
    other,
    base,
    gain,
    local,
    forth,
    back,
    pooled,
    pre,
):
    core, g, chip = place[0], place[1], place[2]
    weight = jnp.concatenate(
        [recv[:, 128:192, :].reshape(2048, LANES), recv[:, 192:256, :].reshape(2048, LANES)],
        axis=1,
    )
    project(normed, edges[...], weight, pre, False)
    half = jnp.where(g == 0, 1, jnp.where(g == 1, 2, jnp.where(g == 2, 4, 8)))
    rows = lax.broadcasted_iota(jnp.int32, (BLOCK, BLOCK), 0)
    cols = lax.broadcasted_iota(jnp.int32, (BLOCK, BLOCK), 1)
    lane = lax.broadcasted_iota(jnp.int32, (BLOCK, LANES), 1)
    for b, (step, total, start) in enumerate(decays(core, raw, own, other, base)):
        at = b * BLOCK
        here = pl.ds(at, BLOCK)

        def taken(offset):
            return pre[HALO + at + offset : HALO + at + offset + BLOCK, LANES:]

        plain = taken(0)
        two = taken(-1) + plain
        four = two + taken(-2) + taken(1)
        eight = four + taken(-4) + taken(-3) + taken(2) + taken(3)
        wide = eight
        for offset in (-8, -7, -6, -5, 4, 5, 6, 7):
            wide = wide + taken(offset)
        window = jnp.where(g == 0, two, jnp.where(g == 1, four, jnp.where(g == 2, eight, wide)))
        token = chip * CHUNK + at + lax.broadcasted_iota(jnp.int32, (BLOCK, LANES), 0)
        count = jnp.minimum(token + half, TOKEN_TOTAL) - jnp.maximum(token - half, 0)
        pooled[here, :] = (window / count.astype(f32) - plain).astype(bf16)

        gate = silu(pre[HALO + at : HALO + at + BLOCK, 0:LANES].astype(bf16).astype(f32))
        gate = gate * gain[...].astype(f32)
        values = (inputs[here, :].astype(f32) * step).astype(bf16)
        writers = jnp.where(core == 0, mine[here, :], theirs[here, :])
        readers = jnp.where(core == 0, theirs[here, :], mine[here, :])
        scores = dot_nt(readers, writers)
        total_t = total.T
        start_t = start.T
        result = jnp.zeros((BLOCK, LANES), f32)
        for h in range(2):
            k = h * 64
            gap = jnp.where(
                cols < rows,
                total[:, k : k + 1] - total_t[k : k + 1, :],
                start_t[k : k + 1, :] - start[:, k : k + 1],
            )
            spread = jnp.exp(jnp.minimum(gap, 0.0))
            spread = jnp.where(cols == rows, 2.0, spread)
            part = jnp.where((lane < 64) == (h == 0), values, jnp.zeros((), bf16))
            result = result + dot((scores * spread).astype(bf16), part)
        local[here, :] = result * gate
        forth[here, :] = jnp.exp(total) * gate
        back[here, :] = jnp.exp(total[BLOCK - 1 : BLOCK, :] - start) * gate


def enter_kernel(
    place, recv, mine, theirs, local, forth, back, totals, ahead, behind, pooled, gain, out
):
    decays = []
    for j in range(CHIPS):
        decays.append(jnp.sum(recv[j, LANES : LANES + 8, :].astype(f32), axis=0, keepdims=True))
    entering = jnp.zeros((LANES, LANES), f32)
    for j in range(CHIPS):
        used = jnp.where(j < place[2], 1.0, 0.0)
        entering = entering * jnp.exp(decays[j] * used) + recv[j, 0:LANES, :].astype(f32) * used
    leaving = jnp.zeros((LANES, LANES), f32)
    for j in reversed(range(CHIPS)):
        used = jnp.where(j > place[2], 1.0, 0.0)
        leaving = leaving * jnp.exp(decays[j] * used) + recv[j, 0:LANES, :].astype(f32) * used
    before = [jnp.zeros((1, LANES), f32)]
    for b in range(BLOCKS):
        before.append(before[-1] + totals[b : b + 1, :])
    for b in range(BLOCKS):
        here = pl.ds(b * BLOCK, BLOCK)
        left = (ahead[b] + entering * jnp.exp(before[b])).astype(bf16)
        right = (behind[b] + leaving * jnp.exp(before[BLOCKS] - before[b + 1])).astype(bf16)
        readers = jnp.where(place[0] == 0, theirs[here, :], mine[here, :])
        both = dot(readers, jnp.concatenate([left, right], axis=1))
        gated = (
            local[here, :]
            + both[:, :LANES] * forth[here, :]
            + both[:, LANES:] * back[here, :]
        ).astype(bf16)
        for k in range(BLOCK // LANES):
            slot = b * (BLOCK // LANES) + k
            out[slot, 0:LANES, :] = gated[k * LANES : (k + 1) * LANES, :]
            out[slot, LANES : 2 * LANES, :] = pooled[slot * LANES : (slot + 1) * LANES, :]
            out[slot, 2 * LANES :, :] = jnp.broadcast_to(gain[...], (8, LANES))


def last_kernel(recv, weight, out, buffer, flags):
    width = 2048 // STEPS

    def copy(k):
        return pltpu.make_async_copy(
            weight.at[:, pl.ds(k * width, width), :], buffer.at[k], flags.at[k]
        )

    for k in range(STEPS):
        copy(k).start()
    gated = [recv[j, 0:LANES, :] for j in range(8)]
    pooled = [recv[j, LANES : 2 * LANES, :] for j in range(8)]
    squares = jnp.zeros((LANES, LANES), f32)
    for j in range(8):
        gain = recv[j, 2 * LANES : 2 * LANES + 8, :].astype(f32)[0:1]
        wide = gated[j].astype(f32) / gain
        squares = squares + wide * wide
    squares = jnp.sum(squares, axis=1, keepdims=True)
    factor = lax.rsqrt(squares / SSD_INNER + EPSILON)
    for k in range(STEPS):
        copy(k).wait()
        state = 0.0
        pool = 0.0
        for x in range(4):
            state = state + dot_nt(
                jnp.concatenate([gated[x], gated[4 + x]], axis=1), buffer[k, x, :, 0:256]
            )
            pool = pool + dot_nt(
                jnp.concatenate([pooled[x], pooled[4 + x]], axis=1), buffer[k, x, :, 256:512]
            )
        out[:, k * width : (k + 1) * width] = (state * factor + pool).astype(bf16)


def shards(
    tokens,
    input_norm_gain,
    gate_matrix,
    input_matrix,
    write_matrix,
    read_matrix,
    step_matrix,
    pooling_input_matrix,
    input_conv_taps,
    write_conv_taps,
    read_conv_taps,
    head_step_base,
    position_step_factor,
    position_log_decay,
    gated_norm_gain,
    group_linear_maps,
    pooling_channel_scale,
    state_output_matrix,
    pooling_output_matrix,
):
    core = lax.axis_index("c")
    group = lax.axis_index("x")
    chip = lax.axis_index(("z", "y"))
    place = jnp.stack([core, group, chip]).astype(jnp.int32)
    swap = [(0, 1), (1, 0)]

    columns = jnp.concatenate([state_output_matrix.T, pooling_output_matrix.T], axis=1)
    out_weight = lax.all_gather(columns, ("x", "z", "y", "c"), axis=0, tiled=True)
    out_weight = out_weight.reshape(4, 2048, 512)

    (whole,) = call(
        prepare_kernel,
        [((32, 264, LANES), bf16)],
        (
            place,
            input_matrix,
            write_matrix,
            read_matrix,
            gate_matrix,
            pooling_input_matrix,
            group_linear_maps,
            pooling_channel_scale[None],
            step_matrix.T,
        ),
        "prepare",
        scratch=[pltpu.VMEM((16, 64), f32)],
        far=(1, 2, 3, 4, 5, 6),
        far_outs=(0,),
    )
    recv_a = lax.all_to_all(whole, ("z", "y", "c"), 0, 0, tiled=True)

    other = lax.ppermute(tokens, "c", swap)
    up = [(i, i + 1) for i in range(CHIPS - 1)]
    down = [(i + 1, i) for i in range(CHIPS - 1)]
    last = jnp.where(core == 0, other[LOCAL - HALO :], tokens[LOCAL - HALO :])
    head = jnp.where(core == 0, tokens[:HALO], other[:HALO])
    before = lax.ppermute(last, ("z", "y"), up)
    after = lax.ppermute(head, ("z", "y"), down)
    (normed,) = call(
        norm_kernel,
        [((CHUNK, 2048), bf16)],
        (place, tokens, other, input_norm_gain[None]),
        "norm",
        far=(1, 2),
        far_outs=(0,),
    )
    places = jnp.concatenate(
        [position_log_decay.T, position_step_factor[None], jnp.zeros((3, LOCAL), f32)], axis=0
    )
    other_places = lax.ppermute(places, "c", swap)
    base = jnp.repeat(lax.dynamic_slice_in_dim(head_step_base, core * 2, 2, 0), 64)[None]
    gain = lax.dynamic_slice_in_dim(gated_norm_gain, core * LANES, LANES, 0)[None]
    taps_in = lax.dynamic_slice_in_dim(input_conv_taps, core * LANES, LANES, 1)
    taps_wr = jnp.where(core == 0, write_conv_taps, read_conv_taps)
    taps = jnp.concatenate([taps_in, taps_wr], axis=1).astype(f32)
    recv_a, normed, places, other_places, base, taps = lax.optimization_barrier(
        (recv_a, normed, places, other_places, base, taps)
    )

    inputs, mine, raw, again, later, edges = call(
        first_kernel,
        [
            ((CHUNK, LANES), bf16),
            ((CHUNK, LANES), bf16),
            ((CHUNK, LANES), f32),
            ((CHUNK, LANES), bf16),
            ((CHUNK, LANES), f32),
            ((2 * HALO, 2048), bf16),
        ],
        (
            pltpu.with_memory_space_constraint(normed, pltpu.HBM),
            recv_a,
            taps,
            before,
            after,
            input_norm_gain[None],
        ),
        "first",
        smem=0,
        scratch=[
            pltpu.VMEM((ROWS, 256), f32),
            pltpu.VMEM((CHUNK, 2048), bf16),
            pltpu.SemaphoreType.DMA((BLOCKS,)),
        ],
        near=(1,),
        raw_in=(0,),
        far_outs=(3, 4, 5),
    )
    theirs = lax.ppermute(mine, "c", swap)
    scaled, totals = call(
        decay_kernel,
        [((CHUNK, 256), bf16), ((8, LANES), f32)],
        (place, inputs, raw, places, other_places, base),
        "decay",
        near=(1, 2),
    )
    slots, ahead, behind = call(
        state_kernel,
        [
            ((CHIPS, LANES + 8, LANES), bf16),
            ((BLOCKS, LANES, LANES), f32),
            ((BLOCKS, LANES, LANES), f32),
        ],
        (place, mine, theirs, scaled, totals),
        "states",
        near=(1, 2, 3, 4),
        far_outs=(0, 1, 2),
    )
    recv_state = lax.all_to_all(slots, ("z", "y"), 0, 0, tiled=True)
    local, forth, back, pooled = call(
        middle_kernel,
        [
            ((CHUNK, LANES), f32),
            ((CHUNK, LANES), f32),
            ((CHUNK, LANES), f32),
            ((CHUNK, LANES), bf16),
        ],
        (
            place,
            normed,
            edges,
            recv_a,
            mine,
            theirs,
            again,
            later,
            places,
            other_places,
            base,
            gain,
        ),
        "middle",
        scratch=[pltpu.VMEM((ROWS, 256), f32)],
        near=(3, 4, 5),
        far=(1, 2, 6, 7),
        far_outs=(0, 1, 2, 3),
    )
    (sent,) = call(
        enter_kernel,
        [((8, 2 * LANES + 8, LANES), bf16)],
        (
            place,
            recv_state,
            mine,
            theirs,
            local,
            forth,
            back,
            totals,
            ahead,
            behind,
            pooled,
            gain,
        ),
        "enter",
        near=(1, 2, 3, 7),
        far=(4, 5, 6, 8, 9, 10),
        far_outs=(0,),
    )
    recv = lax.all_to_all(sent, ("c", "x"), 0, 0, tiled=True)
    return pl.pallas_call(
        last_kernel,
        out_shape=jax.ShapeDtypeStruct((LANES, 2048), bf16),
        in_specs=[VMEM, pl.BlockSpec(memory_space=pltpu.HBM)],
        out_specs=VMEM,
        scratch_shapes=[
            pltpu.VMEM((STEPS, 4, 2048 // STEPS, 512), bf16),
            pltpu.SemaphoreType.DMA((STEPS,)),
        ],
        name="last",
        compiler_params=pltpu.CompilerParams(vmem_limit_bytes=24 * 1024 * 1024),
    )(
        pltpu.with_memory_space_constraint(recv, pltpu.VMEM),
        pltpu.with_memory_space_constraint(out_weight, pltpu.HBM),
    )


def solution(mesh):
    split = Mesh(mesh.devices.reshape(4, 4, 2, 4), ("z", "y", "c", "x"))
    sp = ("z", "y", "c")
    placed = (
        P(sp, None),
        P(),
        P(sp, "x"),
        P(sp, "x"),
        P(sp, "x"),
        P(sp, "x"),
        P(sp, None),
        P(sp, "x"),
        P(None, "x"),
        P(None, "x"),
        P(None, "x"),
        P("x"),
        P(sp),
        P(sp, "x"),
        P("x"),
        P("x", None, None),
        P("x"),
        P("x", sp),
        P("x", sp),
    )
    return jax.shard_map(
        shards,
        mesh=split,
        in_specs=placed,
        out_specs=P(("z", "y", "c", "x"), None),
        check_vma=False,
    )
```

```python
import jax
import jax.numpy as jnp
from jax import lax
from jax.experimental import pallas as pl
from jax.experimental.pallas import tpu as pltpu
from jax.sharding import Mesh, PartitionSpec as P

EPSILON = 1e-06
SSD_INNER = 1024
TOKEN_TOTAL = 16384
LOCAL = 512
CHUNK = 1024
HALO = 8
ROWS = CHUNK + 2 * HALO
BLOCK = 256
BLOCKS = CHUNK // BLOCK
LANES = 128
CHIPS = 16
STEPS = 8
PIECE = 256 * 1024
FINE = 64

f32 = jnp.float32
bf16 = jnp.bfloat16


VMEM = pl.BlockSpec(memory_space=pltpu.VMEM)
SMEM = pl.BlockSpec(memory_space=pltpu.SMEM)


def cuts(array):
    rows = array.shape[0]
    total = array.size * array.dtype.itemsize
    count = 1
    while count * PIECE < total and rows % (2 * count) == 0 and (
        len(array.shape) > 2 or rows // (2 * count) % 16 == 0
    ):
        count *= 2
    return [pl.ds(k * (rows // count), rows // count) for k in range(count)]


def call(kernel, outs, args, name, smem=1, scratch=(), near=(), far=(), far_outs=(), raw_in=(), raw_out=(), late=False):
    n_in, n_out = len(args), len(outs)
    far, far_outs = tuple(far), tuple(far_outs)
    placed = []
    for i, a in enumerate(args):
        if i in near:
            a = pltpu.with_memory_space_constraint(a, pltpu.VMEM)
        elif i in far:
            a = pltpu.with_memory_space_constraint(a, pltpu.HBM)
        placed.append(a)
    hbm = pl.BlockSpec(memory_space=pltpu.HBM)

    def body(*refs):
        ins, rest = list(refs[:n_in]), refs[n_in:]
        results, rest = list(rest[:n_out]), rest[n_out:]
        own, rest = rest[: len(scratch)], rest[len(scratch) :]
        spaces, flags = rest[:-1], rest[-1]
        copies, backs, flag = [], [], 0
        for k, i in enumerate(far):
            for here in cuts(args[i]):
                copies.append(
                    pltpu.make_async_copy(ins[i].at[here], spaces[k].at[here], flags.at[flag])
                )
                flag += 1
            ins[i] = spaces[k]
        for c in copies:
            c.start()
        for k, i in enumerate(far_outs):
            space = spaces[len(far) + k]
            for here in cuts(jax.ShapeDtypeStruct(*outs[i])):
                backs.append(
                    pltpu.make_async_copy(space.at[here], results[i].at[here], flags.at[flag])
                )
                flag += 1
            results[i] = space
        def arrive():
            for c in copies:
                c.wait()

        if late:
            kernel(arrive, *ins, *results, *own)
        else:
            arrive()
            kernel(*ins, *results, *own)
        for c in backs:
            c.start()
        for c in backs:
            c.wait()

    n_flags = sum(len(cuts(args[i])) for i in far)
    n_flags += sum(len(cuts(jax.ShapeDtypeStruct(*outs[i]))) for i in far_outs)
    spaces = [pltpu.VMEM(args[i].shape, args[i].dtype) for i in far]
    spaces += [pltpu.VMEM(*outs[i]) for i in far_outs]
    return pl.pallas_call(
        body,
        out_shape=[
            pltpu.HBM(s, d) if i in far_outs or i in raw_out else pltpu.VMEM(s, d)
            for i, (s, d) in enumerate(outs)
        ],
        in_specs=[
            SMEM if i < smem else hbm if i in far or i in raw_in else VMEM
            for i in range(n_in)
        ],
        out_specs=[hbm if i in far_outs or i in raw_out else VMEM for i in range(n_out)],
        scratch_shapes=list(scratch)
        + spaces
        + [pltpu.SemaphoreType.DMA((max(1, n_flags),))],
        name=name,
        compiler_params=pltpu.CompilerParams(vmem_limit_bytes=24 * 1024 * 1024),
    )(*placed)


def dot(a, b):
    return lax.dot_general(a, b, (((1,), (0,)), ((), ())), preferred_element_type=f32)


def dot_nt(a, b):
    return lax.dot_general(a, b, (((1,), (1,)), ((), ())), preferred_element_type=f32)


def dot_tn(a, b):
    return lax.dot_general(a, b, (((0,), (0,)), ((), ())), preferred_element_type=f32)


def pieces(value):
    high = value.astype(bf16)
    rest = value - high.astype(f32)
    mid = rest.astype(bf16)
    low = (rest - mid.astype(f32)).astype(bf16)
    return high, mid, low


def silu(value):
    return value / (1.0 + jnp.exp(-value))


def prepare_kernel(
    place, inputs, write, read, gates, pools, maps, scale, steps, sent, turned
):
    core, group = place[0], place[1]
    turned[...] = steps[...].astype(f32)
    folded = dot(pools[...], maps[0])
    wide = scale[...].astype(f32)
    wide = jnp.concatenate([wide[0:1], wide[1:2]], axis=1)
    folded = (folded * wide).astype(bf16)
    row = lax.broadcasted_iota(jnp.int32, (8, LANES), 0)
    lane = lax.broadcasted_iota(jnp.int32, (8, LANES), 1)
    for c in range(2):
        at = group * 4 + 2 * c
        here = slice(c * LANES, (c + 1) * LANES)
        pair = [jnp.concatenate([turned[pl.ds(at + h, 1), :]] * 2, axis=1) for h in range(2)]
        tail = jnp.where(row == 0, pair[0], jnp.where(row == 1, pair[1], 0.0))
        tail = jnp.where((lane < 64) == (core == 0), tail, 0.0).astype(bf16)
        for j in range(CHIPS):
            sent[2 * j + c, 0:64, :] = inputs[:, here]
            sent[2 * j + c, 64:128, :] = (write, read)[c][...]
            sent[2 * j + c, 128:192, :] = gates[:, here]
            sent[2 * j + c, 192:256, :] = folded[:, here]
            sent[2 * j + c, 256:264, :] = tail


def normal(rows, scale):
    wide = rows.astype(f32)
    mean = jnp.mean(wide * wide, axis=1, keepdims=True)
    return (wide * lax.rsqrt(mean + EPSILON) * scale).astype(bf16)


def norm_kernel(place, own, other, gain, out):
    core = place[0]
    scale = gain[...].astype(f32)

    def body(k, carry):
        for source, half in ((own, core), (other, 1 - core)):
            rows = normal(source[pl.ds(pl.multiple_of(k * 64, 64), 64), :], scale)
            here = pl.ds(pl.multiple_of(half * LOCAL + k * 64, 64), 64)
            out[here, :] = rows
        return carry

    lax.fori_loop(0, LOCAL // 64, body, 0)


def project(normed, edges, weight, pre, rounded, copies=(), beside=None):
    def keep(value):
        return value.astype(bf16).astype(f32) if rounded else value

    for at in range(0, CHUNK, BLOCK):
        for c in copies[at // FINE : (at + BLOCK) // FINE]:
            c.wait()
        pre[HALO + at : HALO + at + BLOCK, :] = keep(dot(normed[at : at + BLOCK, :], weight))
        if beside is not None:
            beside(at)
    edge = keep(dot(edges()[...], weight))
    pre[0:HALO, :] = edge[0:HALO]
    pre[HALO + CHUNK :, :] = edge[HALO:]


def first_kernel(
    arrive,
    source,
    recv,
    taps,
    before,
    after,
    gain,
    inputs,
    mine,
    raw,
    again,
    later,
    edges,
    pre,
    normed,
    rim,
    flags,
    sends,
):
    copies = [
        pltpu.make_async_copy(
            source.at[pl.ds(at, FINE), :], normed.at[pl.ds(at, FINE), :], flags.at[at // FINE]
        )
        for at in range(0, CHUNK, FINE)
    ]
    for c in copies:
        c.start()
    weight = jnp.concatenate(
        [recv[:, 0:64, :].reshape(2048, LANES), recv[:, 64:128, :].reshape(2048, LANES)], axis=1
    )
    steps = recv[:, 256:264, :].astype(f32).reshape(16, 2, 8, LANES)
    steps = steps[:, 0] + steps[:, 1]
    steps = jnp.concatenate([steps[k] for k in range(16)], axis=1)
    left = lax.broadcasted_iota(jnp.int32, (16, LANES), 1) < 64

    def steps_of(at):
        for here in range(at, at + BLOCK, 16):
            rows = normed[here : here + 16, :].astype(f32)
            pair = [jnp.sum(rows * steps[h : h + 1, :], axis=1, keepdims=True) for h in range(2)]
            raw[here : here + 16, :] = jnp.where(left, pair[0], pair[1])

    def rim_rows():
        arrive()
        rows = jnp.concatenate([before[...], after[...]], axis=0)
        rim[...] = normal(rows, gain[...].astype(f32))
        return rim

    project(normed, rim_rows, weight, pre, True, copies, steps_of)
    backs = [pltpu.make_async_copy(rim, edges, sends.at[2 * BLOCKS])]
    backs[0].start()
    for at in range(0, CHUNK, BLOCK):
        out = (
            pre[HALO - 1 + at : HALO - 1 + at + BLOCK, :] * taps[0:1, :]
            + pre[HALO + at : HALO + at + BLOCK, :] * taps[1:2, :]
            + pre[HALO + 1 + at : HALO + 1 + at + BLOCK, :] * taps[2:3, :]
        )
        out = silu(out).astype(bf16)
        inputs[at : at + BLOCK, :] = out[:, :LANES]
        for k, (near, away) in enumerate(((raw, later), (inputs, again))):
            here = pl.ds(at, BLOCK)
            backs.append(
                pltpu.make_async_copy(
                    near.at[here, :], away.at[here, :], sends.at[2 * (at // BLOCK) + k]
                )
            )
            backs[-1].start()
        mine[at : at + BLOCK, :] = out[:, LANES:]
    for c in backs:
        c.wait()


def decays(core, bases, raw, own, other):
    lane = lax.broadcasted_iota(jnp.int32, (BLOCK, LANES), 1)
    rows = lax.broadcasted_iota(jnp.int32, (BLOCK, BLOCK), 0)
    cols = lax.broadcasted_iota(jnp.int32, (BLOCK, BLOCK), 1)
    lower = jnp.where(cols <= rows, 1.0, 0.0).astype(bf16)
    base = jnp.where(lane < 64, bases[2 * core], bases[2 * core + 1])
    places = [jnp.where(core == 0, own[...], other[...]), jnp.where(core == 0, other[...], own[...])]
    places = [p.T for p in places]
    for at in range(0, CHUNK, BLOCK):
        position = places[at // LOCAL][at % LOCAL : at % LOCAL + BLOCK, :]
        falls = jnp.where(core == 0, position[:, 0:2], position[:, 2:4])
        r = raw[at : at + BLOCK, :]
        soft = jnp.maximum(r, 0.0) + jnp.log1p(jnp.exp(-jnp.abs(r)))
        step = base * soft * position[:, 4:5]
        fall = jnp.where(lane < 64, falls[:, 0:1], falls[:, 1:2]) - step
        total = sum(dot(lower, piece) for piece in pieces(fall))
        yield step, total, total - fall


def decay_kernel(place, bases, inputs, raw, own, other, scaled, totals):
    sums = []
    for b, (step, total, start) in enumerate(decays(place[0], bases, raw, own, other)):
        here = pl.ds(b * BLOCK, BLOCK)
        end = total[BLOCK - 1 : BLOCK, :]
        value = inputs[here, :].astype(f32) * step
        scaled[here, 0:LANES] = (value * jnp.exp(end - total)).astype(bf16)
        scaled[here, LANES:] = (value * jnp.exp(start)).astype(bf16)
        sums.append(end)
    totals[...] = jnp.concatenate(sums + [jnp.zeros((8 - BLOCKS, LANES), f32)], axis=0)


def state_kernel(place, mine, theirs, scaled, totals, slots):
    parts = []
    for b in range(BLOCKS):
        here = pl.ds(b * BLOCK, BLOCK)
        writers = jnp.where(place[0] == 0, mine[here, :], theirs[here, :])
        parts.append(dot_tn(writers, scaled[here, :]))
    state = jnp.zeros((LANES, LANES), f32)
    for b in range(BLOCKS):
        state = state * jnp.exp(totals[b : b + 1, :]) + parts[b][:, :LANES]
    back = jnp.zeros((LANES, LANES), f32)
    for b in reversed(range(BLOCKS)):
        back = back * jnp.exp(totals[b : b + 1, :]) + parts[b][:, LANES:]
    total = totals[0:1, :]
    for b in range(1, BLOCKS):
        total = total + totals[b : b + 1, :]
    row = lax.broadcasted_iota(jnp.int32, (8, LANES), 0)
    high, mid, low = (p.astype(f32) for p in pieces(total))
    tail = jnp.where(row == 0, high, jnp.where(row == 1, mid, jnp.where(row == 2, low, 0.0)))
    tail = tail.astype(bf16)
    state = state.astype(bf16)
    back = back.astype(bf16)
    for j in range(CHIPS):
        slots[j, 0:LANES, :] = jnp.where(j > place[2], state, back)
        slots[j, LANES : LANES + 8, :] = tail


def middle_kernel(
    place,
    bases,
    normed,
    edges,
    recv,
    mine,
    theirs,
    inputs,
    raw,
    own,
    other,
    gain,
    local,
    forth,
    back,
    pooled,
    pre,
):
    core, g, chip = place[0], place[1], place[2]
    weight = jnp.concatenate(
        [recv[:, 128:192, :].reshape(2048, LANES), recv[:, 192:256, :].reshape(2048, LANES)],
        axis=1,
    )
    project(normed, lambda: edges, weight, pre, False)
    half = jnp.where(g == 0, 1, jnp.where(g == 1, 2, jnp.where(g == 2, 4, 8)))
    rows = lax.broadcasted_iota(jnp.int32, (BLOCK, BLOCK), 0)
    cols = lax.broadcasted_iota(jnp.int32, (BLOCK, BLOCK), 1)
    lane = lax.broadcasted_iota(jnp.int32, (BLOCK, LANES), 1)
    parts, fades, results, ahead_gates, back_gates = [], [], [], [], []
    gain_here = jnp.where(core == 0, gain[0:1, :], gain[1:2, :])
    for b, (step, total, start) in enumerate(decays(core, bases, raw, own, other)):
        at = b * BLOCK
        here = pl.ds(at, BLOCK)

        def taken(offset):
            return pre[HALO + at + offset : HALO + at + offset + BLOCK, LANES:]

        plain = taken(0)
        two = taken(-1) + plain
        four = two + taken(-2) + taken(1)
        eight = four + taken(-4) + taken(-3) + taken(2) + taken(3)
        wide = eight
        for offset in (-8, -7, -6, -5, 4, 5, 6, 7):
            wide = wide + taken(offset)
        window = jnp.where(g == 0, two, jnp.where(g == 1, four, jnp.where(g == 2, eight, wide)))
        token = chip * CHUNK + at + lax.broadcasted_iota(jnp.int32, (BLOCK, LANES), 0)
        count = jnp.minimum(token + half, TOKEN_TOTAL) - jnp.maximum(token - half, 0)
        pooled[here, :] = (window / count.astype(f32) - plain).astype(bf16)

        gate = silu(pre[HALO + at : HALO + at + BLOCK, 0:LANES].astype(bf16).astype(f32))
        gate = gate * gain_here.astype(f32)
        value = inputs[here, :].astype(f32) * step
        values = value.astype(bf16)
        end = total[BLOCK - 1 : BLOCK, :]
        writers = jnp.where(core == 0, mine[here, :], theirs[here, :])
        readers = jnp.where(core == 0, theirs[here, :], mine[here, :])
        scores = dot_nt(readers, writers)
        total_t = total.T
        start_t = start.T
        result = jnp.zeros((BLOCK, LANES), f32)
        for h in range(2):
            k = h * 64
            gap = jnp.where(
                cols < rows,
                total[:, k : k + 1] - total_t[k : k + 1, :],
                start_t[k : k + 1, :] - start[:, k : k + 1],
            )
            spread = jnp.exp(jnp.minimum(gap, 0.0))
            spread = jnp.where(cols == rows, 2.0, spread)
            part = jnp.where((lane < 64) == (h == 0), values, jnp.zeros((), bf16))
            result = result + dot((scores * spread).astype(bf16), part)
        onward = (value * jnp.exp(end - total)).astype(bf16)
        backward = (value * jnp.exp(start)).astype(bf16)
        parts.append(dot_tn(writers, jnp.concatenate([onward, backward], axis=1)))
        fades.append(jnp.exp(end))
        results.append(result * gate)
        ahead_gates.append(jnp.exp(total) * gate)
        back_gates.append(jnp.exp(end - start) * gate)
        forth[here, :] = ahead_gates[-1].astype(bf16)
        back[here, :] = back_gates[-1].astype(bf16)
    zero = jnp.zeros((LANES, LANES), f32)
    ahead, behind = [zero], [zero]
    for b in range(BLOCKS - 1):
        ahead.append(ahead[-1] * fades[b] + parts[b][:, :LANES])
    for b in reversed(range(1, BLOCKS)):
        behind.append(behind[-1] * fades[b] + parts[b][:, LANES:])
    behind = behind[::-1]
    for b in range(BLOCKS):
        here = pl.ds(b * BLOCK, BLOCK)
        readers = jnp.where(core == 0, theirs[here, :], mine[here, :])
        carried = jnp.concatenate([ahead[b], behind[b]], axis=1).astype(bf16)
        both = dot(readers, carried)
        local[here, :] = (
            results[b] + both[:, :LANES] * ahead_gates[b] + both[:, LANES:] * back_gates[b]
        ).astype(bf16)
    pooled[CHUNK:, :] = jnp.broadcast_to(gain_here, (8, LANES))


def enter_kernel(
    arrive, place, recv, mine, theirs, local, forth, back, totals, pooled, out
):
    decays = []
    for j in range(CHIPS):
        decays.append(jnp.sum(recv[j, LANES : LANES + 8, :].astype(f32), axis=0, keepdims=True))
    entering = jnp.zeros((LANES, LANES), f32)
    for j in range(CHIPS):
        used = jnp.where(j < place[2], 1.0, 0.0)
        entering = entering * jnp.exp(decays[j] * used) + recv[j, 0:LANES, :].astype(f32) * used
    leaving = jnp.zeros((LANES, LANES), f32)
    for j in reversed(range(CHIPS)):
        used = jnp.where(j > place[2], 1.0, 0.0)
        leaving = leaving * jnp.exp(decays[j] * used) + recv[j, 0:LANES, :].astype(f32) * used
    arrive()
    before = [jnp.zeros((1, LANES), f32)]
    for b in range(BLOCKS):
        before.append(before[-1] + totals[b : b + 1, :])
    for b in range(BLOCKS):
        here = pl.ds(b * BLOCK, BLOCK)
        left = (entering * jnp.exp(before[b])).astype(bf16)
        right = (leaving * jnp.exp(before[BLOCKS] - before[b + 1])).astype(bf16)
        readers = jnp.where(place[0] == 0, theirs[here, :], mine[here, :])
        both = dot(readers, jnp.concatenate([left, right], axis=1))
        gated = (
            local[here, :].astype(f32)
            + both[:, :LANES] * forth[here, :].astype(f32)
            + both[:, LANES:] * back[here, :].astype(f32)
        ).astype(bf16)
        for k in range(BLOCK // LANES):
            slot = b * (BLOCK // LANES) + k
            out[slot, 0:LANES, :] = gated[k * LANES : (k + 1) * LANES, :]
            out[slot, LANES : 2 * LANES, :] = pooled[slot * LANES : (slot + 1) * LANES, :]
            out[slot, 2 * LANES :, :] = pooled[CHUNK:, :]


def last_kernel(recv, weight, out, buffer, sums, flags):
    width = 2048 // STEPS
    copies = [
        pltpu.make_async_copy(
            weight.at[x, pl.ds(k * width, width), :], buffer.at[k, x], flags.at[4 * k + x]
        )
        for k in range(STEPS)
        for x in range(4)
    ]
    for c in copies:
        c.start()
    gated, pooled = [], []
    squares = jnp.zeros((LANES, LANES), f32)
    for x in range(4):
        for j in (x, x + 4):
            part = recv[j, 0:LANES, :]
            gated.append(part)
            pooled.append(recv[j, LANES : 2 * LANES, :])
            gain = recv[j, 2 * LANES : 2 * LANES + 8, :].astype(f32)[0:1]
            wide = part.astype(f32) / gain
            squares = squares + wide * wide
    squares = jnp.sum(squares, axis=1, keepdims=True)
    factor = lax.rsqrt(squares / SSD_INNER + EPSILON)
    gated = jnp.concatenate(gated, axis=1)
    pooled = jnp.concatenate(pooled, axis=1)
    backs = []
    for s in range(STEPS):
        for c in copies[4 * s : 4 * s + 4]:
            c.wait()
        both = [
            jnp.concatenate([buffer[s, x, :, at : at + 256] for x in range(4)], axis=1)
            for at in (0, 256)
        ]
        result = dot_nt(gated, both[0]) * factor + dot_nt(pooled, both[1])
        here = pl.ds(s * width, width)
        sums[:, here] = result.astype(bf16)
        backs.append(
            pltpu.make_async_copy(sums.at[:, here], out.at[:, here], flags.at[4 * STEPS + s])
        )
        backs[-1].start()
    for c in backs:
        c.wait()


def shards(
    tokens,
    input_norm_gain,
    gate_matrix,
    input_matrix,
    write_matrix,
    read_matrix,
    step_matrix,
    pooling_input_matrix,
    input_conv_taps,
    write_conv_taps,
    read_conv_taps,
    head_step_base,
    position_step_factor,
    position_log_decay,
    gated_norm_gain,
    group_linear_maps,
    pooling_channel_scale,
    state_output_matrix,
    pooling_output_matrix,
):
    core = lax.axis_index("c")
    group = lax.axis_index("x")
    chip = lax.axis_index(("z", "y"))
    place = jnp.stack([core, group, chip]).astype(jnp.int32)
    swap = [(0, 1), (1, 0)]

    columns = jnp.concatenate([state_output_matrix.T, pooling_output_matrix.T], axis=1)
    out_weight = lax.all_gather(columns, ("x", "z", "y", "c"), axis=0, tiled=True)
    out_weight = out_weight.reshape(4, 2048, 512)

    (whole,) = call(
        prepare_kernel,
        [((32, 264, LANES), bf16)],
        (
            place,
            input_matrix,
            write_matrix,
            read_matrix,
            gate_matrix,
            pooling_input_matrix,
            group_linear_maps,
            pooling_channel_scale.reshape(2, LANES),
            step_matrix.T,
        ),
        "prepare",
        scratch=[pltpu.VMEM((16, 64), f32)],
        far=(1, 2, 3, 4, 5, 6, 7, 8),
        far_outs=(0,),
    )

    other = lax.ppermute(tokens, "c", swap)
    up = [(i, i + 1) for i in range(CHIPS - 1)]
    down = [(i + 1, i) for i in range(CHIPS - 1)]
    last = jnp.where(core == 0, other[LOCAL - HALO :], tokens[LOCAL - HALO :])
    head = jnp.where(core == 0, tokens[:HALO], other[:HALO])
    before = lax.ppermute(last, ("z", "y"), up)
    after = lax.ppermute(head, ("z", "y"), down)
    (normed,) = call(
        norm_kernel,
        [((CHUNK, 2048), bf16)],
        (place, tokens, other, input_norm_gain[None]),
        "norm",
        near=(3,),
        far=(1, 2),
        far_outs=(0,),
    )
    recv_a = lax.all_to_all(whole, ("z", "y", "c"), 0, 0, tiled=True)
    places = jnp.concatenate(
        [position_log_decay.T, position_step_factor[None], jnp.zeros((3, LOCAL), f32)], axis=0
    )
    other_places = lax.ppermute(places, "c", swap)
    gain = gated_norm_gain.reshape(2, LANES)
    taps_in = lax.dynamic_slice_in_dim(input_conv_taps, core * LANES, LANES, 1)
    taps_wr = jnp.where(core == 0, write_conv_taps, read_conv_taps)
    taps = jnp.concatenate([taps_in, taps_wr], axis=1).astype(f32)
    recv_a, normed, places, other_places, taps = lax.optimization_barrier(
        (recv_a, normed, places, other_places, taps)
    )

    inputs, mine, raw, again, later, edges = call(
        first_kernel,
        [
            ((CHUNK, LANES), bf16),
            ((CHUNK, LANES), bf16),
            ((CHUNK, LANES), f32),
            ((CHUNK, LANES), bf16),
            ((CHUNK, LANES), f32),
            ((2 * HALO, 2048), bf16),
        ],
        (
            pltpu.with_memory_space_constraint(normed, pltpu.HBM),
            recv_a,
            taps,
            before,
            after,
            input_norm_gain[None],
        ),
        "first",
        smem=0,
        scratch=[
            pltpu.VMEM((ROWS, 256), f32),
            pltpu.VMEM((CHUNK, 2048), bf16),
            pltpu.VMEM((2 * HALO, 2048), bf16),
            pltpu.SemaphoreType.DMA((CHUNK // FINE,)),
            pltpu.SemaphoreType.DMA((2 * BLOCKS + 1,)),
        ],
        near=(1, 3, 4, 5),
        raw_in=(0,),
        raw_out=(3, 4, 5),
        late=True,
    )
    theirs = lax.ppermute(mine, "c", swap)
    scaled, totals = call(
        decay_kernel,
        [((CHUNK, 256), bf16), ((8, LANES), f32)],
        (place, head_step_base, inputs, raw, places, other_places),
        "decay",
        smem=2,
        near=(2, 3, 4, 5),
    )
    (slots,) = call(
        state_kernel,
        [((CHIPS, LANES + 8, LANES), bf16)],
        (place, mine, theirs, scaled, totals),
        "states",
        near=(1, 2, 3, 4),
        far_outs=(0,),
    )
    recv_state = lax.all_to_all(slots, ("z", "y"), 0, 0, tiled=True)
    local, forth, back, pooled = call(
        middle_kernel,
        [
            ((CHUNK, LANES), bf16),
            ((CHUNK, LANES), bf16),
            ((CHUNK, LANES), bf16),
            ((CHUNK + 8, LANES), bf16),
        ],
        (
            place,
            head_step_base,
            normed,
            edges,
            recv_a,
            mine,
            theirs,
            again,
            later,
            places,
            other_places,
            gain,
        ),
        "middle",
        scratch=[pltpu.VMEM((ROWS, 256), f32)],
        smem=2,
        near=(4, 5, 6, 9, 10),
        far=(2, 3, 7, 8, 11),
        far_outs=(0, 1, 2, 3),
    )
    (sent,) = call(
        enter_kernel,
        [((8, 2 * LANES + 8, LANES), bf16)],
        (
            place,
            recv_state,
            mine,
            theirs,
            local,
            forth,
            back,
            totals,
            pooled,
        ),
        "enter",
        near=(1, 2, 3, 7),
        far=(4, 5, 6, 8),
        late=True,
    )
    recv = lax.all_to_all(sent, ("c", "x"), 0, 0, tiled=True)
    return pl.pallas_call(
        last_kernel,
        out_shape=jax.ShapeDtypeStruct((LANES, 2048), bf16),
        in_specs=[VMEM, pl.BlockSpec(memory_space=pltpu.HBM)],
        out_specs=pl.BlockSpec(memory_space=pltpu.HBM),
        scratch_shapes=[
            pltpu.VMEM((STEPS, 4, 2048 // STEPS, 512), bf16),
            pltpu.VMEM((LANES, 2048), bf16),
            pltpu.SemaphoreType.DMA((5 * STEPS,)),
        ],
        name="last",
        compiler_params=pltpu.CompilerParams(vmem_limit_bytes=24 * 1024 * 1024),
    )(
        pltpu.with_memory_space_constraint(recv, pltpu.VMEM),
        pltpu.with_memory_space_constraint(out_weight, pltpu.HBM),
    )


def solution(mesh):
    split = Mesh(mesh.devices.reshape(4, 4, 2, 4), ("z", "y", "c", "x"))
    sp = ("z", "y", "c")
    placed = (
        P(sp, None),
        P(),
        P(sp, "x"),
        P(sp, "x"),
        P(sp, "x"),
        P(sp, "x"),
        P(sp, None),
        P(sp, "x"),
        P(None, "x"),
        P(None, "x"),
        P(None, "x"),
        P("x"),
        P(sp),
        P(sp, "x"),
        P("x"),
        P("x", None, None),
        P("x"),
        P("x", sp),
        P("x", sp),
    )
    return jax.shard_map(
        shards,
        mesh=split,
        in_specs=placed,
        out_specs=P(("z", "y", "c", "x"), None),
        check_vma=False,
    )
```

```python
import jax
import jax.numpy as jnp
from jax import lax
from jax.experimental import pallas as pl
from jax.experimental.pallas import tpu as pltpu
from jax.sharding import Mesh, PartitionSpec as P

EPSILON = 1e-06
SSD_INNER = 1024
TOKEN_TOTAL = 16384
LOCAL = 512
CHUNK = 1024
HALO = 8
ROWS = CHUNK + 2 * HALO
BLOCK = 256
BLOCKS = CHUNK // BLOCK
LANES = 128
CHIPS = 16
STEPS = 8
PIECE = 256 * 1024
FINE = 64

f32 = jnp.float32
bf16 = jnp.bfloat16


VMEM = pl.BlockSpec(memory_space=pltpu.VMEM)
SMEM = pl.BlockSpec(memory_space=pltpu.SMEM)


def cuts(array):
    rows = array.shape[0]
    total = array.size * array.dtype.itemsize
    count = 1
    while count * PIECE < total and rows % (2 * count) == 0 and (
        len(array.shape) > 2 or rows // (2 * count) % 16 == 0
    ):
        count *= 2
    return [pl.ds(k * (rows // count), rows // count) for k in range(count)]


def call(kernel, outs, args, name, smem=1, scratch=(), near=(), far=(), far_outs=(), raw_in=(), raw_out=(), late=False):
    n_in, n_out = len(args), len(outs)
    far, far_outs = tuple(far), tuple(far_outs)
    placed = []
    for i, a in enumerate(args):
        if i in near:
            a = pltpu.with_memory_space_constraint(a, pltpu.VMEM)
        elif i in far:
            a = pltpu.with_memory_space_constraint(a, pltpu.HBM)
        placed.append(a)
    hbm = pl.BlockSpec(memory_space=pltpu.HBM)

    def body(*refs):
        ins, rest = list(refs[:n_in]), refs[n_in:]
        results, rest = list(rest[:n_out]), rest[n_out:]
        own, rest = rest[: len(scratch)], rest[len(scratch) :]
        spaces, flags = rest[:-1], rest[-1]
        copies, backs, flag = [], [], 0
        for k, i in enumerate(far):
            for here in cuts(args[i]):
                copies.append(
                    pltpu.make_async_copy(ins[i].at[here], spaces[k].at[here], flags.at[flag])
                )
                flag += 1
            ins[i] = spaces[k]
        for c in copies:
            c.start()
        for k, i in enumerate(far_outs):
            space = spaces[len(far) + k]
            for here in cuts(jax.ShapeDtypeStruct(*outs[i])):
                backs.append(
                    pltpu.make_async_copy(space.at[here], results[i].at[here], flags.at[flag])
                )
                flag += 1
            results[i] = space
        def arrive():
            for c in copies:
                c.wait()

        if late:
            kernel(arrive, *ins, *results, *own)
        else:
            arrive()
            kernel(*ins, *results, *own)
        for c in backs:
            c.start()
        for c in backs:
            c.wait()

    n_flags = sum(len(cuts(args[i])) for i in far)
    n_flags += sum(len(cuts(jax.ShapeDtypeStruct(*outs[i]))) for i in far_outs)
    spaces = [pltpu.VMEM(args[i].shape, args[i].dtype) for i in far]
    spaces += [pltpu.VMEM(*outs[i]) for i in far_outs]
    return pl.pallas_call(
        body,
        out_shape=[
            pltpu.HBM(s, d) if i in far_outs or i in raw_out else pltpu.VMEM(s, d)
            for i, (s, d) in enumerate(outs)
        ],
        in_specs=[
            SMEM if i < smem else hbm if i in far or i in raw_in else VMEM
            for i in range(n_in)
        ],
        out_specs=[hbm if i in far_outs or i in raw_out else VMEM for i in range(n_out)],
        scratch_shapes=list(scratch)
        + spaces
        + [pltpu.SemaphoreType.DMA((max(1, n_flags),))],
        name=name,
        compiler_params=pltpu.CompilerParams(vmem_limit_bytes=24 * 1024 * 1024),
    )(*placed)


def dot(a, b):
    return lax.dot_general(a, b, (((1,), (0,)), ((), ())), preferred_element_type=f32)


def dot_nt(a, b):
    return lax.dot_general(a, b, (((1,), (1,)), ((), ())), preferred_element_type=f32)


def dot_tn(a, b):
    return lax.dot_general(a, b, (((0,), (0,)), ((), ())), preferred_element_type=f32)


def pieces(value):
    high = value.astype(bf16)
    rest = value - high.astype(f32)
    mid = rest.astype(bf16)
    low = (rest - mid.astype(f32)).astype(bf16)
    return high, mid, low


def silu(value):
    return value / (1.0 + jnp.exp(-value))


def prepare_kernel(
    place, inputs, write, read, gates, pools, maps, scale, steps, sent, turned
):
    core, group = place[0], place[1]
    turned[...] = steps[...].astype(f32)
    folded = dot(pools[...], maps[0])
    wide = scale[...].astype(f32)
    wide = jnp.concatenate([wide[0:1], wide[1:2]], axis=1)
    folded = (folded * wide).astype(bf16)
    row = lax.broadcasted_iota(jnp.int32, (8, LANES), 0)
    lane = lax.broadcasted_iota(jnp.int32, (8, LANES), 1)
    for c in range(2):
        at = group * 4 + 2 * c
        here = slice(c * LANES, (c + 1) * LANES)
        pair = [jnp.concatenate([turned[pl.ds(at + h, 1), :]] * 2, axis=1) for h in range(2)]
        tail = jnp.where(row == 0, pair[0], jnp.where(row == 1, pair[1], 0.0))
        tail = jnp.where((lane < 64) == (core == 0), tail, 0.0).astype(bf16)
        for j in range(CHIPS):
            sent[2 * j + c, 0:64, :] = inputs[:, here]
            sent[2 * j + c, 64:128, :] = (write, read)[c][...]
            sent[2 * j + c, 128:192, :] = gates[:, here]
            sent[2 * j + c, 192:256, :] = folded[:, here]
            sent[2 * j + c, 256:264, :] = tail


def normal(rows, scale):
    wide = rows.astype(f32)
    mean = jnp.mean(wide * wide, axis=1, keepdims=True)
    return (wide * lax.rsqrt(mean + EPSILON) * scale).astype(bf16)


def norm_kernel(place, own, other, gain, out):
    core = place[0]
    scale = gain[...].astype(f32)

    def body(k, carry):
        for source, half in ((own, core), (other, 1 - core)):
            rows = normal(source[pl.ds(pl.multiple_of(k * 64, 64), 64), :], scale)
            here = pl.ds(pl.multiple_of(half * LOCAL + k * 64, 64), 64)
            out[here, :] = rows
        return carry

    lax.fori_loop(0, LOCAL // 64, body, 0)


def project(normed, edges, weight, pre, rounded, copies=(), beside=None):
    def keep(value):
        return value.astype(bf16).astype(f32) if rounded else value

    for at in range(0, CHUNK, BLOCK):
        for c in copies[at // FINE : (at + BLOCK) // FINE]:
            c.wait()
        pre[HALO + at : HALO + at + BLOCK, :] = keep(dot(normed[at : at + BLOCK, :], weight))
        if beside is not None:
            beside(at)
    edge = keep(dot(edges()[...], weight))
    pre[0:HALO, :] = edge[0:HALO]
    pre[HALO + CHUNK :, :] = edge[HALO:]


def first_kernel(
    arrive,
    source,
    recv,
    taps,
    before,
    after,
    gain,
    inputs,
    mine,
    raw,
    again,
    later,
    edges,
    pre,
    normed,
    rim,
    flags,
    sends,
):
    copies = [
        pltpu.make_async_copy(
            source.at[pl.ds(at, FINE), :], normed.at[pl.ds(at, FINE), :], flags.at[at // FINE]
        )
        for at in range(0, CHUNK, FINE)
    ]
    for c in copies:
        c.start()
    weight = jnp.concatenate(
        [recv[:, 0:64, :].reshape(2048, LANES), recv[:, 64:128, :].reshape(2048, LANES)], axis=1
    )
    steps = recv[:, 256:264, :].astype(f32).reshape(16, 2, 8, LANES)
    steps = steps[:, 0] + steps[:, 1]
    steps = jnp.concatenate([steps[k] for k in range(16)], axis=1)
    left = lax.broadcasted_iota(jnp.int32, (16, LANES), 1) < 64

    def steps_of(at):
        for here in range(at, at + BLOCK, 16):
            rows = normed[here : here + 16, :].astype(f32)
            pair = [jnp.sum(rows * steps[h : h + 1, :], axis=1, keepdims=True) for h in range(2)]
            raw[here : here + 16, :] = jnp.where(left, pair[0], pair[1])

    def rim_rows():
        arrive()
        rows = jnp.concatenate([before[...], after[...]], axis=0)
        rim[...] = normal(rows, gain[...].astype(f32))
        return rim

    project(normed, rim_rows, weight, pre, True, copies, steps_of)
    backs = [pltpu.make_async_copy(rim, edges, sends.at[2 * BLOCKS])]
    backs[0].start()
    for at in range(0, CHUNK, BLOCK):
        out = (
            pre[HALO - 1 + at : HALO - 1 + at + BLOCK, :] * taps[0:1, :]
            + pre[HALO + at : HALO + at + BLOCK, :] * taps[1:2, :]
            + pre[HALO + 1 + at : HALO + 1 + at + BLOCK, :] * taps[2:3, :]
        )
        out = silu(out).astype(bf16)
        inputs[at : at + BLOCK, :] = out[:, :LANES]
        for k, (near, away) in enumerate(((raw, later), (inputs, again))):
            here = pl.ds(at, BLOCK)
            backs.append(
                pltpu.make_async_copy(
                    near.at[here, :], away.at[here, :], sends.at[2 * (at // BLOCK) + k]
                )
            )
            backs[-1].start()
        mine[at : at + BLOCK, :] = out[:, LANES:]
    for c in backs:
        c.wait()


def decays(core, bases, raw, own, other):
    lane = lax.broadcasted_iota(jnp.int32, (BLOCK, LANES), 1)
    rows = lax.broadcasted_iota(jnp.int32, (BLOCK, BLOCK), 0)
    cols = lax.broadcasted_iota(jnp.int32, (BLOCK, BLOCK), 1)
    lower = jnp.where(cols <= rows, 1.0, 0.0).astype(bf16)
    base = jnp.where(lane < 64, bases[2 * core], bases[2 * core + 1])
    places = [jnp.where(core == 0, own[...], other[...]), jnp.where(core == 0, other[...], own[...])]
    places = [p.T for p in places]
    for at in range(0, CHUNK, BLOCK):
        position = places[at // LOCAL][at % LOCAL : at % LOCAL + BLOCK, :]
        falls = jnp.where(core == 0, position[:, 0:2], position[:, 2:4])
        r = raw[at : at + BLOCK, :]
        soft = jnp.maximum(r, 0.0) + jnp.log1p(jnp.exp(-jnp.abs(r)))
        step = base * soft * position[:, 4:5]
        fall = jnp.where(lane < 64, falls[:, 0:1], falls[:, 1:2]) - step
        total = sum(dot(lower, piece) for piece in pieces(fall))
        yield step, total, total - fall


def decay_kernel(place, bases, inputs, raw, own, other, scaled, totals):
    sums = []
    for b, (step, total, start) in enumerate(decays(place[0], bases, raw, own, other)):
        here = pl.ds(b * BLOCK, BLOCK)
        end = total[BLOCK - 1 : BLOCK, :]
        value = inputs[here, :].astype(f32) * step
        scaled[here, 0:LANES] = (value * jnp.exp(end - total)).astype(bf16)
        scaled[here, LANES:] = (value * jnp.exp(start)).astype(bf16)
        sums.append(end)
    totals[...] = jnp.concatenate(sums + [jnp.zeros((8 - BLOCKS, LANES), f32)], axis=0)


def state_kernel(place, mine, theirs, scaled, totals, slots):
    parts = []
    for b in range(BLOCKS):
        here = pl.ds(b * BLOCK, BLOCK)
        writers = jnp.where(place[0] == 0, mine[here, :], theirs[here, :])
        parts.append(dot_tn(writers, scaled[here, :]))
    state = jnp.zeros((LANES, LANES), f32)
    for b in range(BLOCKS):
        state = state * jnp.exp(totals[b : b + 1, :]) + parts[b][:, :LANES]
    back = jnp.zeros((LANES, LANES), f32)
    for b in reversed(range(BLOCKS)):
        back = back * jnp.exp(totals[b : b + 1, :]) + parts[b][:, LANES:]
    total = totals[0:1, :]
    for b in range(1, BLOCKS):
        total = total + totals[b : b + 1, :]
    row = lax.broadcasted_iota(jnp.int32, (8, LANES), 0)
    high, mid, low = (p.astype(f32) for p in pieces(total))
    tail = jnp.where(row == 0, high, jnp.where(row == 1, mid, jnp.where(row == 2, low, 0.0)))
    tail = tail.astype(bf16)
    state = state.astype(bf16)
    back = back.astype(bf16)
    for j in range(CHIPS):
        slots[j, 0:LANES, :] = jnp.where(j > place[2], state, back)
        slots[j, LANES : LANES + 8, :] = tail


def middle_kernel(
    place,
    bases,
    normed,
    edges,
    recv,
    mine,
    theirs,
    inputs,
    raw,
    own,
    other,
    gain,
    local,
    forth,
    back,
    pooled,
    pre,
):
    core, g, chip = place[0], place[1], place[2]
    weight = jnp.concatenate(
        [recv[:, 128:192, :].reshape(2048, LANES), recv[:, 192:256, :].reshape(2048, LANES)],
        axis=1,
    )
    project(normed, lambda: edges, weight, pre, False)
    half = jnp.where(g == 0, 1, jnp.where(g == 1, 2, jnp.where(g == 2, 4, 8)))
    rows = lax.broadcasted_iota(jnp.int32, (BLOCK, BLOCK), 0)
    cols = lax.broadcasted_iota(jnp.int32, (BLOCK, BLOCK), 1)
    lane = lax.broadcasted_iota(jnp.int32, (BLOCK, LANES), 1)
    parts, fades, results, ahead_gates, back_gates = [], [], [], [], []
    gain_here = jnp.where(core == 0, gain[0:1, :], gain[1:2, :])
    for b, (step, total, start) in enumerate(decays(core, bases, raw, own, other)):
        at = b * BLOCK
        here = pl.ds(at, BLOCK)

        def taken(offset):
            return pre[HALO + at + offset : HALO + at + offset + BLOCK, LANES:]

        plain = taken(0)
        two = taken(-1) + plain
        four = two + taken(-2) + taken(1)
        eight = four + taken(-4) + taken(-3) + taken(2) + taken(3)
        wide = eight
        for offset in (-8, -7, -6, -5, 4, 5, 6, 7):
            wide = wide + taken(offset)
        window = jnp.where(g == 0, two, jnp.where(g == 1, four, jnp.where(g == 2, eight, wide)))
        token = chip * CHUNK + at + lax.broadcasted_iota(jnp.int32, (BLOCK, LANES), 0)
        count = jnp.minimum(token + half, TOKEN_TOTAL) - jnp.maximum(token - half, 0)
        pooled[here, :] = (window / count.astype(f32) - plain).astype(bf16)

        gate = silu(pre[HALO + at : HALO + at + BLOCK, 0:LANES].astype(bf16).astype(f32))
        gate = gate * gain_here.astype(f32)
        value = inputs[here, :].astype(f32) * step
        values = value.astype(bf16)
        end = total[BLOCK - 1 : BLOCK, :]
        writers = jnp.where(core == 0, mine[here, :], theirs[here, :])
        readers = jnp.where(core == 0, theirs[here, :], mine[here, :])
        scores = dot_nt(readers, writers)
        total_t = total.T
        start_t = start.T
        result = jnp.zeros((BLOCK, LANES), f32)
        for h in range(2):
            k = h * 64
            gap = jnp.where(
                cols < rows,
                total[:, k : k + 1] - total_t[k : k + 1, :],
                start_t[k : k + 1, :] - start[:, k : k + 1],
            )
            spread = jnp.exp(jnp.minimum(gap, 0.0))
            spread = jnp.where(cols == rows, 2.0, spread)
            part = jnp.where((lane < 64) == (h == 0), values, jnp.zeros((), bf16))
            result = result + dot((scores * spread).astype(bf16), part)
        onward = (value * jnp.exp(end - total)).astype(bf16)
        backward = (value * jnp.exp(start)).astype(bf16)
        parts.append(dot_tn(writers, jnp.concatenate([onward, backward], axis=1)))
        fades.append(jnp.exp(end))
        results.append(result * gate)
        ahead_gates.append(jnp.exp(total) * gate)
        back_gates.append(jnp.exp(end - start) * gate)
        forth[here, :] = ahead_gates[-1].astype(bf16)
        back[here, :] = back_gates[-1].astype(bf16)
    zero = jnp.zeros((LANES, LANES), f32)
    ahead, behind = [zero], [zero]
    for b in range(BLOCKS - 1):
        ahead.append(ahead[-1] * fades[b] + parts[b][:, :LANES])
    for b in reversed(range(1, BLOCKS)):
        behind.append(behind[-1] * fades[b] + parts[b][:, LANES:])
    behind = behind[::-1]
    for b in range(BLOCKS):
        here = pl.ds(b * BLOCK, BLOCK)
        readers = jnp.where(core == 0, theirs[here, :], mine[here, :])
        carried = jnp.concatenate([ahead[b], behind[b]], axis=1).astype(bf16)
        both = dot(readers, carried)
        local[here, :] = (
            results[b] + both[:, :LANES] * ahead_gates[b] + both[:, LANES:] * back_gates[b]
        ).astype(bf16)
    pooled[CHUNK:, :] = jnp.broadcast_to(gain_here, (8, LANES))


def enter_kernel(
    arrive, place, recv, mine, theirs, local, forth, back, totals, pooled, out
):
    decays = []
    for j in range(CHIPS):
        decays.append(jnp.sum(recv[j, LANES : LANES + 8, :].astype(f32), axis=0, keepdims=True))
    entering = jnp.zeros((LANES, LANES), f32)
    for j in range(CHIPS):
        used = jnp.where(j < place[2], 1.0, 0.0)
        entering = entering * jnp.exp(decays[j] * used) + recv[j, 0:LANES, :].astype(f32) * used
    leaving = jnp.zeros((LANES, LANES), f32)
    for j in reversed(range(CHIPS)):
        used = jnp.where(j > place[2], 1.0, 0.0)
        leaving = leaving * jnp.exp(decays[j] * used) + recv[j, 0:LANES, :].astype(f32) * used
    arrive()
    before = [jnp.zeros((1, LANES), f32)]
    for b in range(BLOCKS):
        before.append(before[-1] + totals[b : b + 1, :])
    for b in range(BLOCKS):
        here = pl.ds(b * BLOCK, BLOCK)
        left = (entering * jnp.exp(before[b])).astype(bf16)
        right = (leaving * jnp.exp(before[BLOCKS] - before[b + 1])).astype(bf16)
        readers = jnp.where(place[0] == 0, theirs[here, :], mine[here, :])
        both = dot(readers, jnp.concatenate([left, right], axis=1))
        gated = (
            local[here, :].astype(f32)
            + both[:, :LANES] * forth[here, :].astype(f32)
            + both[:, LANES:] * back[here, :].astype(f32)
        ).astype(bf16)
        for k in range(BLOCK // LANES):
            slot = b * (BLOCK // LANES) + k
            out[slot, 0:LANES, :] = gated[k * LANES : (k + 1) * LANES, :]
            out[slot, LANES : 2 * LANES, :] = pooled[slot * LANES : (slot + 1) * LANES, :]
            out[slot, 2 * LANES :, :] = pooled[CHUNK:, :]


def last_kernel(recv, weight, out, buffer, sums, flags):
    per = CHIPS // STEPS
    width = LANES * per
    copies = [
        pltpu.make_async_copy(
            weight.at[x, pl.ds(k * per, per)], buffer.at[k, x], flags.at[4 * k + x]
        )
        for k in range(STEPS)
        for x in range(4)
    ]
    for c in copies:
        c.start()
    gated, pooled = [], []
    squares = jnp.zeros((LANES, LANES), f32)
    for x in range(4):
        for j in (x, x + 4):
            part = recv[j, 0:LANES, :]
            gated.append(part)
            pooled.append(recv[j, LANES : 2 * LANES, :])
            gain = recv[j, 2 * LANES : 2 * LANES + 8, :].astype(f32)[0:1]
            wide = part.astype(f32) / gain
            squares = squares + wide * wide
    squares = jnp.sum(squares, axis=1, keepdims=True)
    factor = lax.rsqrt(squares / SSD_INNER + EPSILON)
    gated = jnp.concatenate(gated, axis=1)
    pooled = jnp.concatenate(pooled, axis=1)
    backs = []
    for s in range(STEPS):
        for c in copies[4 * s : 4 * s + 4]:
            c.wait()
        both = [
            jnp.concatenate(
                [
                    jnp.concatenate([buffer[s, x, k, part] for k in range(per)], axis=1)
                    for x in range(4)
                ],
                axis=0,
            )
            for part in range(2)
        ]
        result = dot(gated, both[0]) * factor + dot(pooled, both[1])
        here = pl.ds(s * width, width)
        sums[:, here] = result.astype(bf16)
        backs.append(
            pltpu.make_async_copy(sums.at[:, here], out.at[:, here], flags.at[4 * STEPS + s])
        )
        backs[-1].start()
    for c in backs:
        c.wait()


def shards(
    tokens,
    input_norm_gain,
    gate_matrix,
    input_matrix,
    write_matrix,
    read_matrix,
    step_matrix,
    pooling_input_matrix,
    input_conv_taps,
    write_conv_taps,
    read_conv_taps,
    head_step_base,
    position_step_factor,
    position_log_decay,
    gated_norm_gain,
    group_linear_maps,
    pooling_channel_scale,
    state_output_matrix,
    pooling_output_matrix,
):
    core = lax.axis_index("c")
    group = lax.axis_index("x")
    chip = lax.axis_index(("z", "y"))
    place = jnp.stack([core, group, chip]).astype(jnp.int32)
    swap = [(0, 1), (1, 0)]

    kept = jnp.where(core == 0, state_output_matrix, pooling_output_matrix)
    taken = jnp.where(core == 0, pooling_output_matrix, state_output_matrix)
    taken = lax.ppermute(taken, "c", swap)
    columns = jnp.concatenate(
        [jnp.where(core == 0, kept, taken), jnp.where(core == 0, taken, kept)], axis=1
    )
    out_weight = lax.all_gather(columns, ("x", "z", "y", "c"), axis=0, tiled=True)
    out_weight = out_weight.reshape(4, CHIPS, 2, 256, LANES)

    (whole,) = call(
        prepare_kernel,
        [((32, 264, LANES), bf16)],
        (
            place,
            input_matrix,
            write_matrix,
            read_matrix,
            gate_matrix,
            pooling_input_matrix,
            group_linear_maps,
            pooling_channel_scale.reshape(2, LANES),
            step_matrix.T,
        ),
        "prepare",
        scratch=[pltpu.VMEM((16, 64), f32)],
        far=(1, 2, 3, 4, 5, 6, 7, 8),
        far_outs=(0,),
    )

    other = lax.ppermute(tokens, "c", swap)
    up = [(i, i + 1) for i in range(CHIPS - 1)]
    down = [(i + 1, i) for i in range(CHIPS - 1)]
    last = jnp.where(core == 0, other[LOCAL - HALO :], tokens[LOCAL - HALO :])
    head = jnp.where(core == 0, tokens[:HALO], other[:HALO])
    before = lax.ppermute(last, ("z", "y"), up)
    after = lax.ppermute(head, ("z", "y"), down)
    (normed,) = call(
        norm_kernel,
        [((CHUNK, 2048), bf16)],
        (place, tokens, other, input_norm_gain[None]),
        "norm",
        near=(3,),
        far=(1, 2),
        far_outs=(0,),
    )
    recv_a = lax.all_to_all(whole, ("z", "y", "c"), 0, 0, tiled=True)
    places = jnp.concatenate(
        [position_log_decay.T, position_step_factor[None], jnp.zeros((3, LOCAL), f32)], axis=0
    )
    other_places = lax.ppermute(places, "c", swap)
    gain = gated_norm_gain.reshape(2, LANES)
    taps_in = lax.dynamic_slice_in_dim(input_conv_taps, core * LANES, LANES, 1)
    taps_wr = jnp.where(core == 0, write_conv_taps, read_conv_taps)
    taps = jnp.concatenate([taps_in, taps_wr], axis=1).astype(f32)
    recv_a, normed, places, other_places, taps = lax.optimization_barrier(
        (recv_a, normed, places, other_places, taps)
    )

    inputs, mine, raw, again, later, edges = call(
        first_kernel,
        [
            ((CHUNK, LANES), bf16),
            ((CHUNK, LANES), bf16),
            ((CHUNK, LANES), f32),
            ((CHUNK, LANES), bf16),
            ((CHUNK, LANES), f32),
            ((2 * HALO, 2048), bf16),
        ],
        (
            pltpu.with_memory_space_constraint(normed, pltpu.HBM),
            recv_a,
            taps,
            before,
            after,
            input_norm_gain[None],
        ),
        "first",
        smem=0,
        scratch=[
            pltpu.VMEM((ROWS, 256), f32),
            pltpu.VMEM((CHUNK, 2048), bf16),
            pltpu.VMEM((2 * HALO, 2048), bf16),
            pltpu.SemaphoreType.DMA((CHUNK // FINE,)),
            pltpu.SemaphoreType.DMA((2 * BLOCKS + 1,)),
        ],
        near=(1, 3, 4, 5),
        raw_in=(0,),
        raw_out=(3, 4, 5),
        late=True,
    )
    theirs = lax.ppermute(mine, "c", swap)
    scaled, totals = call(
        decay_kernel,
        [((CHUNK, 256), bf16), ((8, LANES), f32)],
        (place, head_step_base, inputs, raw, places, other_places),
        "decay",
        smem=2,
        near=(2, 3, 4, 5),
    )
    (slots,) = call(
        state_kernel,
        [((CHIPS, LANES + 8, LANES), bf16)],
        (place, mine, theirs, scaled, totals),
        "states",
        near=(1, 2, 3, 4),
        far_outs=(0,),
    )
    recv_state = lax.all_to_all(slots, ("z", "y"), 0, 0, tiled=True)
    local, forth, back, pooled = call(
        middle_kernel,
        [
            ((CHUNK, LANES), bf16),
            ((CHUNK, LANES), bf16),
            ((CHUNK, LANES), bf16),
            ((CHUNK + 8, LANES), bf16),
        ],
        (
            place,
            head_step_base,
            normed,
            edges,
            recv_a,
            mine,
            theirs,
            again,
            later,
            places,
            other_places,
            gain,
        ),
        "middle",
        scratch=[pltpu.VMEM((ROWS, 256), f32)],
        smem=2,
        near=(4, 5, 6, 9, 10),
        far=(2, 3, 7, 8, 11),
        far_outs=(0, 1, 2, 3),
    )
    (sent,) = call(
        enter_kernel,
        [((8, 2 * LANES + 8, LANES), bf16)],
        (
            place,
            recv_state,
            mine,
            theirs,
            local,
            forth,
            back,
            totals,
            pooled,
        ),
        "enter",
        near=(1, 2, 3, 7),
        far=(4, 5, 6, 8),
        late=True,
    )
    recv = lax.all_to_all(sent, ("c", "x"), 0, 0, tiled=True)
    return pl.pallas_call(
        last_kernel,
        out_shape=jax.ShapeDtypeStruct((LANES, 2048), bf16),
        in_specs=[VMEM, pl.BlockSpec(memory_space=pltpu.HBM)],
        out_specs=pl.BlockSpec(memory_space=pltpu.HBM),
        scratch_shapes=[
            pltpu.VMEM((STEPS, 4, CHIPS // STEPS, 2, 256, LANES), bf16),
            pltpu.VMEM((LANES, 2048), bf16),
            pltpu.SemaphoreType.DMA((5 * STEPS,)),
        ],
        name="last",
        compiler_params=pltpu.CompilerParams(vmem_limit_bytes=24 * 1024 * 1024),
    )(
        pltpu.with_memory_space_constraint(recv, pltpu.VMEM),
        pltpu.with_memory_space_constraint(out_weight, pltpu.HBM),
    )


def solution(mesh):
    split = Mesh(mesh.devices.reshape(4, 4, 2, 4), ("z", "y", "c", "x"))
    sp = ("z", "y", "c")
    placed = (
        P(sp, None),
        P(),
        P(sp, "x"),
        P(sp, "x"),
        P(sp, "x"),
        P(sp, "x"),
        P(sp, None),
        P(sp, "x"),
        P(None, "x"),
        P(None, "x"),
        P(None, "x"),
        P("x"),
        P(sp),
        P(sp, "x"),
        P("x"),
        P("x", None, None),
        P("x"),
        P("x", sp),
        P("x", sp),
    )
    return jax.shard_map(
        shards,
        mesh=split,
        in_specs=placed,
        out_specs=P(("z", "y", "c", "x"), None),
        check_vma=False,
    )
```
